32 devices in a mesh: sp: 8 (over z, x), tp: 4 (over y, core).
Axes of the slice: x: 2, y: 2, z: 4, core: 2. Of those that a mesh axis runs over, the one named last changes fastest.
Arguments:
- query_one: bfloat16 [1024, 1024], P('sp', 'tp'), may hold values from -100 to 100
- key_one: bfloat16 [1024, 512], P('sp', 'tp'), may hold values from -10 to 10
- query_two: bfloat16 [1024, 1024], P('sp', 'tp'), may hold values from -100 to 100
- key_two: bfloat16 [1024, 512], P('sp', 'tp'), may hold values from -10 to 10
- value: bfloat16 [1024, 1024], P('sp', 'tp'), may hold values from -6 to 6
- lambda_head: float32 [8], P('tp'), may hold values from 0.3 to 0.8
- head_gain: float32 [256], replicated, may hold values from 0.1 to 1.9
- out_weight: bfloat16 [2048, 4096], P('tp'), may hold values from -0.125 to 0.125
- residual: bfloat16 [1024, 4096], P(('sp', 'tp')), may hold values from -6 to 6
- norm_gain: float32 [4096], replicated, may hold values from 0.1 to 1.9
- route_expert: int32 [1024, 2], P(('sp', 'tp')), may hold values from 0 to 7, all different within a row; in each aligned block of 32 rows (0 to 31, 32 to 63, ...) at most 16 rows name the same one
- route_weight: float32 [1024, 2], P(('sp', 'tp')), may hold values from 0.1 to 0.9
- expert_gate: bfloat16 [8, 4096, 1024], P('sp', None, 'tp'), may hold values from -0.09375 to 0.09375
- expert_up: bfloat16 [8, 4096, 1024], P('sp', None, 'tp'), may hold values from -0.09375 to 0.09375
- expert_down: bfloat16 [8, 1024, 4096], P('sp', 'tp'), may hold values from -0.1875 to 0.1875
Outputs:
- output: bfloat16 [1024, 4096], P(('sp', 'tp'))
The draws below stay inside these ranges and needn't reach their ends.
Inputs may be any that keep to these rules, and one draw needn't show every extreme that they name: `route_expert`: the 2 entries of a row differ. In each aligned block of 32 rows (the rows of one device) no expert is named more than 16 times, a bound that some block reaches.
All inputs are finite; a program needn't handle non-finite values.
Results may differ from the reference program's by a relative error of at most 0.015.
Values may be sent and summed in bfloat16 or wider, within the bound.
A program may use at most 128 MiB of HBM per device.

```python
import math
import jax
import jax.numpy as jnp
import numpy as np
from jax import lax

D = 4096
HEADS = 8
KV_HEADS = 4
HEAD = 128
EXPERT_FF = 1024
TOP = 2
TOKENS = 1024
ROWS_DEV = 32
EXPERTS = 8
CAP = 16
FF_PART = 256
N_TP = 4


def drawn(key, which):
    folded = jax.random.fold_in(key, which)
    query_key, key_key = jax.random.split(folded)
    key_rows = jnp.clip(1.3 * jax.random.normal(key_key, (TOKENS, KV_HEADS * HEAD), jnp.float32), -7.8, 7.8)
    query_rows = jnp.clip(1.3 * jax.random.normal(query_key, (TOKENS, HEADS * HEAD), jnp.float32), -7.8, 7.8)
    return (query_rows, key_rows)


def draw_query_one(key, part):
    return drawn(key, 11)[0].astype(jnp.bfloat16)


def draw_key_one(key, part):
    return drawn(key, 11)[1].astype(jnp.bfloat16)


def draw_query_two(key, part):
    return drawn(key, 23)[0].astype(jnp.bfloat16)


def draw_key_two(key, part):
    return drawn(key, 23)[1].astype(jnp.bfloat16)


def levels(rng, shape, shards, low, high):
    factor_of, own = 1.0, jax.random.fold_in(rng, 6)
    for position, parts in shards:
        draws = jnp.exp(jax.random.uniform(jax.random.fold_in(own, position), (parts,), jnp.float32, low / len(shards), high / len(shards)))
        factor_of = factor_of * jnp.repeat(draws, shape[position] // parts).reshape([-1 if axis == position else 1 for axis in range(len(shape))])
    return factor_of


def shared_out(key, own, number, rows, count, top, most, skew):
    ranking = jax.random.permutation(key, count)
    heavy_load, ordinary = load_shares(count, rows * top, most, skew, True), load_shares(count, rows * top, most, skew, False)
    places = jnp.arange(count)

    def named(sizes, turn):
        used = int((sizes > 0).sum())
        fixed = max(1, used // 4)
        moved = fixed + (places - fixed + turn * (used - fixed)) % max(1, count - fixed)
        return jnp.zeros((count,), jnp.int32).at[ranking[jnp.where(places < fixed, places, moved)]].set(jnp.asarray(sizes, jnp.int32))

    sizes = jnp.where(number % 4 == 0, named(heavy_load, number // 4), named(ordinary, number - number // 4 - 1))
    mixed = jax.random.permutation(jax.random.fold_in(own, 3), count)
    donor, taker = mixed[0:count // 2 * 2:2], mixed[1:count // 2 * 2:2]
    slack = jnp.minimum(sizes[donor] - 1, most - sizes[taker]) // 2
    slack = jnp.where((donor == ranking[0]) | (taker == ranking[0]) | (sizes[taker] == 0), 0, jnp.maximum(slack, 0))
    moved = jax.random.randint(jax.random.fold_in(own, 4), (count // 2,), 0, 1 << 20) % (slack + 1)
    sizes = sizes.at[donor].add(-moved).at[taker].add(moved)
    members = jnp.searchsorted(jnp.cumsum(sizes), jnp.arange(rows * top), side="right").astype(jnp.int32)
    listing = members.reshape(top, rows).T
    listing = listing[jax.random.permutation(jax.random.fold_in(own, 1), rows)]
    turn = jax.random.randint(jax.random.fold_in(own, 2), (rows, 1), 0, top)
    return jnp.take_along_axis(listing, (jnp.arange(top)[None, :] + turn) % top, axis=1)


def load_shares(count, total, limit, lean, full):
    portions = [(1 << 20) // math.isqrt(grade ** lean) + 1 for grade in range(1, count + 1)]
    largest = limit if full else min(limit, max(-(-total // count), total * portions[0] // sum(portions)))
    least = 1 if total - largest >= count - 1 else 0
    given, rest = [largest] + [least] * (count - 1), total - largest - least * (count - 1)
    while rest > 0:
        free = [i for i in range(1, count) if given[i] < largest] or [i for i in range(1, count) if given[i] < limit]
        pool, remaining = sum([portions[i] for i in free]), rest
        for i in free:
            more = min(limit - given[i], max(1, remaining * portions[i] // pool), rest)
            given[i] = given[i] + more
            rest = rest - more
    return np.array(given)


def scatter_about(stream_key, shape, spread, limit, pieces=(), kind=jnp.bfloat16):
    values = spread * jax.random.normal(stream_key, shape, jnp.float32)
    if pieces:
        values = values * levels(stream_key, shape, pieces, -0.22, 0.18)
    return jnp.clip(values, -limit, limit).astype(kind)


def setup_inputs(seed: int = 0) -> dict:
    seeds = jax.random.split(jax.random.key(seed), 16)
    query_one = draw_query_one(jax.random.fold_in(seeds[15], 71), 0)
    key_one = draw_key_one(jax.random.fold_in(seeds[15], 71), 0)
    query_two = draw_query_two(jax.random.fold_in(seeds[15], 71), 0)
    key_two = draw_key_two(jax.random.fold_in(seeds[15], 71), 0)
    value = scatter_about(seeds[4], (TOKENS, KV_HEADS * 2 * HEAD), 1.0, 6.0, ((0, 8), (1, 4)))
    lambda_head = jnp.clip(0.3 + 0.5 * jax.random.uniform(seeds[5], (HEADS,), jnp.float32) ** levels(seeds[5], (HEADS,), ((0, 4),), -0.2, 0.2), 0.3, 0.8)
    head_gain = jnp.clip(1.0 + 0.18 * jax.random.normal(seeds[6], (2 * HEAD,), jnp.float32), 0.1, 1.9)
    out_weight = scatter_about(seeds[7], (HEADS * 2 * HEAD, D), (HEADS * 2 * HEAD) ** -0.5, 0.125, ((0, 4),))
    residual = scatter_about(seeds[8], (TOKENS, D), 1.0, 6.0, ((0, 32),))
    norm_gain = jnp.clip(1.0 + 0.18 * jax.random.normal(seeds[9], (D,), jnp.float32), 0.1, 1.9)
    route_expert_keys = jax.random.split(jax.random.fold_in(seeds[10], 1), TOKENS // ROWS_DEV)
    route_expert_turns = jax.random.permutation(jax.random.fold_in(seeds[10], 3), TOKENS // ROWS_DEV)
    route_expert = jax.vmap(lambda own, number: shared_out(jax.random.fold_in(seeds[10], 2), own, number, ROWS_DEV, EXPERTS, TOP, CAP, 2))(route_expert_keys, route_expert_turns).reshape((TOKENS, TOP))
    route_weight = jnp.clip(0.1 + 0.79999997 * jax.random.uniform(seeds[11], (TOKENS, TOP), jnp.float32) ** levels(seeds[11], (TOKENS, TOP), ((0, 32),), -0.2, 0.2), 0.1, 0.9)
    expert_gate = scatter_about(seeds[12], (EXPERTS, D, EXPERT_FF), D ** -0.5, 0.09375, ((0, 8), (2, 4)))
    expert_up = scatter_about(seeds[13], (EXPERTS, D, EXPERT_FF), D ** -0.5, 0.09375, ((0, 8), (2, 4)))
    expert_down = scatter_about(seeds[14], (EXPERTS, EXPERT_FF, D), EXPERT_FF ** -0.5, 0.1875, ((0, 8), (1, 4)))
    return {"query_one": query_one, "key_one": key_one, "query_two": query_two, "key_two": key_two, "value": value, "lambda_head": lambda_head, "head_gain": head_gain, "out_weight": out_weight, "residual": residual, "norm_gain": norm_gain, "route_expert": route_expert, "route_weight": route_weight, "expert_gate": expert_gate, "expert_up": expert_up, "expert_down": expert_down}


def one_map(queries, key_rows, values, allowed):
    scores = jnp.einsum('qhd,khd->hqk', queries, key_rows) * HEAD ** (-0.5)
    scores = jnp.where(allowed[None], scores, -jnp.inf)
    largest = lax.optimization_barrier(jnp.max(scores, axis=-1, keepdims=True))
    weights = jnp.exp(scores - largest)
    totals = lax.optimization_barrier(jnp.sum(weights, axis=-1))
    rounded = lax.optimization_barrier(weights.astype(jnp.bfloat16)).astype(jnp.float32)
    summed = jnp.einsum('hqk,khe->qhe', rounded, values)
    return summed / jnp.transpose(totals)[:, :, None]

def reference(query_one, key_one, query_two, key_two, value, lambda_head, head_gain, out_weight, residual, norm_gain, route_expert, route_weight, expert_gate, expert_up, expert_down):
    per_key = HEADS // KV_HEADS

    def widen(source, columns):
        shaped = source.astype(jnp.float32).reshape(TOKENS, KV_HEADS, columns)
        return jnp.repeat(shaped, per_key, axis=1)
    key_first = widen(key_one, HEAD)
    key_second = widen(key_two, HEAD)
    values = widen(value, 2 * HEAD)
    block_rows = math.gcd(TOKENS, 256)
    positions = jnp.arange(TOKENS, dtype=jnp.int32)

    def attend(block_start):
        first_map = lax.dynamic_slice_in_dim(query_one, block_start, block_rows, 0)
        first_map = first_map.astype(jnp.float32).reshape(block_rows, HEADS, HEAD)
        second_map = lax.dynamic_slice_in_dim(query_two, block_start, block_rows, 0)
        second_map = second_map.astype(jnp.float32).reshape(block_rows, HEADS, HEAD)
        query_pos = block_start + jnp.arange(block_rows, dtype=jnp.int32)
        allowed = positions[None, :] <= query_pos[:, None]
        out_first = one_map(first_map, key_first, values, allowed)
        out_second = one_map(second_map, key_second, values, allowed)
        difference = out_first - lambda_head[None, :, None] * out_second
        scaled = difference * lax.rsqrt(lax.optimization_barrier(jnp.mean(difference * difference, axis=-1, keepdims=True)) + 1e-05) * head_gain
        return scaled.astype(jnp.bfloat16).reshape(block_rows, HEADS * 2 * HEAD)
    starts = jnp.arange(TOKENS // block_rows, dtype=jnp.int32) * block_rows
    attended = lax.map(attend, starts).reshape(TOKENS, HEADS * 2 * HEAD)
    projected = jnp.dot(attended, out_weight, preferred_element_type=jnp.float32)
    summed_in = residual.astype(jnp.float32) + projected
    centered = summed_in - lax.optimization_barrier(jnp.mean(summed_in, axis=-1, keepdims=True))
    variance = lax.optimization_barrier(jnp.mean(centered * centered, axis=-1, keepdims=True))
    normed = (centered * lax.rsqrt(variance + 1e-05) * norm_gain).astype(jnp.bfloat16)
    pair_count = TOKENS * TOP
    chosen = route_expert.reshape(pair_count)
    onehot = (chosen[:, None] == jnp.arange(EXPERTS, dtype=jnp.int32)[None, :]).astype(jnp.int32)
    rank_in = lax.optimization_barrier(jnp.sum((jnp.cumsum(onehot, axis=0) - onehot) * onehot, axis=1))
    most_rows = CAP * (TOKENS // ROWS_DEV)
    slot_table = jnp.full((EXPERTS, most_rows), pair_count, jnp.int32)
    slot_table = slot_table.at[chosen, rank_in].set(jnp.arange(pair_count, dtype=jnp.int32))

    def expert(expert_id):
        pair_ids = slot_table[expert_id]
        token_rows = normed[jnp.minimum(pair_ids, pair_count - 1) // TOP]
        gated = jnp.dot(token_rows, expert_gate[expert_id], preferred_element_type=jnp.float32)
        upward = jnp.dot(token_rows, expert_up[expert_id], preferred_element_type=jnp.float32)
        hidden = (jax.nn.silu(gated) * upward).astype(jnp.bfloat16)
        accum = jnp.zeros((most_rows, D), jnp.float32)
        for segment in range(N_TP):
            partial_value = jnp.dot(hidden[:, segment * FF_PART:(segment + 1) * FF_PART], expert_down[expert_id, segment * FF_PART:(segment + 1) * FF_PART], preferred_element_type=jnp.float32)
            accum = accum + lax.optimization_barrier(partial_value.astype(jnp.bfloat16)).astype(jnp.float32)
        return accum.astype(jnp.bfloat16)
    results = lax.map(expert, jnp.arange(EXPERTS, dtype=jnp.int32))
    gathered = jnp.zeros((pair_count + 1, D), jnp.bfloat16)
    gathered = gathered.at[slot_table.reshape(-1)].set(results.reshape(EXPERTS * most_rows, D))
    picked = gathered[:pair_count].reshape(TOKENS, TOP, D).astype(jnp.float32)
    combined = lax.optimization_barrier(jnp.sum(route_weight[:, :, None] * picked, axis=1))
    return (normed.astype(jnp.float32) + combined).astype(jnp.bfloat16)
```

```python
import functools
import math

import jax
import jax.numpy as jnp
from jax import lax
from jax.experimental import pallas as pl
from jax.experimental.pallas import tpu as pltpu
from jax.sharding import PartitionSpec as P

HEAD = 128
VMEM_BYTES = 58 * 1024 * 1024
CHUNKS, EARLY = 4, 3


def map_step(carried, query_rows, key_block, value_block, allowed):
    largest, totals, running = carried
    scores = jnp.einsum(
        "qcgd,kcd->cgqk", query_rows, key_block, preferred_element_type=jnp.float32
    ) * HEAD ** (-0.5)
    scores = jnp.where(allowed[None, None], scores, -jnp.inf)
    updated = jnp.maximum(largest, jnp.max(scores, axis=-1))
    weights = jnp.exp(scores - updated[..., None])
    rescale = jnp.exp(largest - updated)
    totals = totals * rescale + jnp.sum(weights, axis=-1)
    added = jnp.einsum(
        "cgqk,kce->qcge",
        weights.astype(jnp.bfloat16),
        value_block,
        preferred_element_type=jnp.float32,
    )
    running = running * jnp.transpose(rescale, (2, 0, 1))[..., None] + added
    return (updated, totals, running)


def finish(carried):
    return carried[2] / jnp.transpose(carried[1], (2, 0, 1))[..., None]


def remote(src, dst, send, recv, sp_to, tp_to):
    return pltpu.make_async_remote_copy(
        src_ref=src,
        dst_ref=dst,
        send_sem=send,
        recv_sem=recv,
        device_id={"sp": sp_to, "tp": tp_to},
        device_id_type=pl.DeviceIdType.MESH,
    )


def flipped(index, mask):
    bit = 1
    while bit <= mask:
        if mask & bit:
            index = index + bit - 2 * bit * lax.rem(lax.div(index, bit), 2)
        bit *= 2
    return index


def layer_kernel(
    sp, tp, heads, kv_heads, cap, early,
    q1_hbm, k1_hbm, q2_hbm, k2_hbm, v_hbm, lam, gain, ow_hbm, res_hbm, ngain,
    route_e, route_w, gate_hbm, up_hbm, down_hbm, out,
    q1, q2, res, kv, ow, att, pbuf, prc, pcs, pry, total, normed, placed, mix,
    gate, up, down, moved, hid, hidr, outg, tok, part, rc, cs, ry, fin, ret,
    f_sem, z_send, z_recv, x_send, x_recv, pc_send, pc_recv, py_send, py_recv,
    d_send, d_recv, h_send, h_recv, a_send, a_recv, y_send, y_recv, c_send, c_recv,
    rc_send, rc_recv, ry_send, ry_recv, ra_send, ra_recv,
):
    s = lax.axis_index("sp")
    t = lax.axis_index("tp")
    z, x = lax.div(s, 2), lax.rem(s, 2)
    y, c = lax.div(t, 2), lax.rem(t, 2)
    lanes = sp // 2
    px = flipped(s, 1)
    core = flipped(t, 1)
    plane_peer = flipped(t, 2)
    corner = flipped(t, 3)
    local = q1.shape[0]
    rows, width = out.shape
    kw = kv_heads * HEAD
    chunks, chunk = moved.shape[0], moved.shape[3]
    shared = chunks * chunk
    own_part = width - shared

    barrier = pltpu.get_barrier_semaphore()
    peers = [(flipped(s, k), t) for k in range(1, sp)]
    peers += [(s, flipped(t, r)) for r in range(1, tp)]
    for sp_to, tp_to in peers:
        pl.semaphore_signal(
            barrier,
            inc=1,
            device_id={"sp": sp_to, "tp": tp_to},
            device_id_type=pl.DeviceIdType.MESH,
        )
    sources = [
        (k1_hbm, kv.at[s, :, 0:kw]), (k2_hbm, kv.at[s, :, kw:2 * kw]),
        (v_hbm, kv.at[s, :, 2 * kw:4 * kw]), (down_hbm, down), (q1_hbm, q1), (q2_hbm, q2),
        (ow_hbm, ow), (res_hbm, res), (gate_hbm, gate), (up_hbm, up),
    ]
    fetches = [
        pltpu.make_async_copy(src, dst, f_sem.at[i]) for i, (src, dst) in enumerate(sources)
    ]
    for copy in fetches:
        copy.start()
    for block in range(1, sp):
        @pl.when(block > s)
        def _():
            kv[block] = jnp.zeros(kv.shape[1:], kv.dtype)

    places = lax.broadcasted_iota(jnp.int32, (sp * cap, rows), 0).astype(jnp.float32)
    owner = jnp.floor((places + 0.5) / cap)
    slot = places - owner * cap
    named = jnp.zeros((sp * cap, rows), jnp.float32)
    share = jnp.zeros((sp * cap, rows), jnp.float32)
    for choice in range(route_e.shape[0]):
        match = route_e[choice:choice + 1, :].astype(jnp.float32) == owner
        named += jnp.where(match, 1.0, 0.0)
        share += jnp.where(match, route_w[choice:choice + 1, :], 0.0)
    earlier = lax.broadcasted_iota(jnp.int32, (rows, rows), 0) < lax.broadcasted_iota(
        jnp.int32, (rows, rows), 1
    )
    rank = jnp.dot(
        named.astype(jnp.bfloat16),
        jnp.where(earlier, 1.0, 0.0).astype(jnp.bfloat16),
        preferred_element_type=jnp.float32,
    )
    held = jnp.where(rank == slot, named, 0.0)
    placed[...] = held.astype(jnp.bfloat16)
    mix[...] = share * held

    sends = []

    def begin(copy):
        copy.start()
        sends.append(copy)

    def along(block, to, d):
        return remote(kv.at[block], kv.at[block], z_send.at[d], z_recv.at[d], to, t)

    def across(block, d):
        return remote(kv.at[block], kv.at[block], x_send.at[d], x_recv.at[d], px, t)

    for copy in fetches[:3]:
        copy.wait()
    pl.semaphore_wait(barrier, len(peers))
    for d in (2, 1):
        @pl.when(z + d < lanes)
        def _():
            along(s, s + 2 * d, d).start()

    @pl.when(x == 0)
    def _():
        across(s, 0).start()

    def lend(n, r):
        to = flipped(t, r)
        columns = slice(n * chunk, (n + 1) * chunk)
        return remote(
            down.at[:, columns], moved.at[n, r - 1], d_send.at[n, r - 1], d_recv.at[n, r - 1],
            s, to,
        )

    def relend(n):
        return remote(
            moved.at[n, 1], moved.at[n, 2], d_send.at[n, 2], d_recv.at[n, 2], s, core
        )

    fetches[3].wait()
    for n in range(early):
        begin(lend(n, 2))
    for n in range(chunks):
        begin(lend(n, 1))

    for level, order in ((1, (1,)), (2, (2, 1)), (3, (1, 2, 3))):
        @pl.when(z == level)
        def _():
            for d in order:
                along(s - 2 * d, s, d).wait_recv()
                if level + d == 4 and d == 2:
                    along(s - 2 * d, s + 2, 3).start()
                across(s - 2 * d, d).start()
            for d in order:
                across(px - 2 * d, d).wait_recv()

    @pl.when(x == 1)
    def _():
        across(px, 0).wait_recv()

    for copy in fetches[4:6]:
        copy.wait()
    length = sp * local
    key_pos = lax.broadcasted_iota(jnp.int32, (local, length), 1)
    query_pos = s * local + lax.broadcasted_iota(jnp.int32, (local, length), 0)
    allowed = key_pos <= query_pos
    per_key = heads // kv_heads
    for h in range(heads):
        g = h // per_key
        values = kv[:, :, 2 * kw + g * 2 * HEAD:2 * kw + (g + 1) * 2 * HEAD]
        values = values.reshape(length, 2 * HEAD)
        maps = []
        for which, q in ((0, q1), (1, q2)):
            start = which * kw + g * HEAD
            keys = kv[:, :, start:start + HEAD].reshape(length, HEAD)
            scores = lax.dot_general(
                q[:, h * HEAD:(h + 1) * HEAD],
                keys,
                (((1,), (1,)), ((), ())),
                preferred_element_type=jnp.float32,
            ) * HEAD ** (-0.5)
            scores = jnp.where(allowed, scores, -1e30)
            weights = jnp.exp(scores - jnp.max(scores, axis=-1, keepdims=True))
            totals = jnp.sum(weights, axis=-1, keepdims=True)
            added = jnp.dot(
                weights.astype(jnp.bfloat16), values, preferred_element_type=jnp.float32
            )
            maps.append(added / totals)
        difference = maps[0] - lam[h] * maps[1]
        scaled = (
            difference
            * lax.rsqrt(jnp.mean(difference * difference, axis=-1, keepdims=True) + 1e-05)
            * gain[...]
        )
        att[:, h * 2 * HEAD:(h + 1) * 2 * HEAD] = scaled.astype(jnp.bfloat16)

    fetches[6].wait()

    def share_pair(there, dy, p):
        group = flipped(core, 2) if dy else core
        return remote(
            pbuf.at[p, group], prc.at[dy, p], pc_send.at[dy, p], pc_recv.at[dy, p], s, core
        )

    def share_plane(p):
        return remote(pcs.at[p], pry.at[p], py_send.at[p], py_recv.at[p], s, plane_peer)

    parts = pbuf.shape[0]
    part_width = width // parts
    for p in range(parts + 1):
        if p < parts:
            piece = jnp.dot(
                att[...],
                ow[:, p * part_width:(p + 1) * part_width],
                preferred_element_type=jnp.float32,
            )
            pbuf[p] = piece.astype(jnp.bfloat16).reshape(tp, rows, part_width)
            for dy in (1, 0):
                begin(share_pair(None, dy, p))
        if p >= 1:
            share_pair(None, 1, p - 1).wait_recv()
            pcs[p - 1] = (
                pbuf[p - 1, plane_peer].astype(jnp.float32) + prc[1, p - 1].astype(jnp.float32)
            ).astype(jnp.bfloat16)
            begin(share_plane(p - 1))
    for n in range(early, chunks):
        begin(lend(n, 2))
    fetches[7].wait()
    summed = jnp.zeros((rows, 1), jnp.float32)
    for p in range(parts):
        columns = slice(p * part_width, (p + 1) * part_width)
        share_pair(None, 0, p).wait_recv()
        piece = pbuf[p, t].astype(jnp.float32) + prc[0, p].astype(jnp.float32)
        piece = piece + res[:, columns].astype(jnp.float32)
        share_plane(p).wait_recv()
        piece = piece + pry[p].astype(jnp.float32)
        total[:, columns] = piece
        summed += jnp.sum(piece, axis=-1, keepdims=True)
    centered = total[...] - summed / width
    variance = jnp.mean(centered * centered, axis=-1, keepdims=True)
    normed[...] = (centered * lax.rsqrt(variance + 1e-05) * ngain[...]).astype(jnp.bfloat16)

    tile = math.gcd(width, 1024)

    @pl.loop(0, width // tile)
    def _(n):
        columns = pl.ds(pl.multiple_of(n * tile, tile), tile)
        piece = jnp.dot(placed[...], normed[:, columns], preferred_element_type=jnp.float32)
        outg[:, :, columns] = piece.astype(jnp.bfloat16).reshape(sp, cap, tile)

    def arrive(k):
        there = flipped(s, k)
        return remote(outg.at[there], tok.at[k, t], a_send.at[k], a_recv.at[k], there, t)

    def plane(k):
        return remote(
            tok.at[k, t], tok.at[k, t], y_send.at[k], y_recv.at[k], s, plane_peer
        )

    def pair(k, dy):
        mine = plane_peer if dy else t
        return remote(
            tok.at[k, mine], tok.at[k, mine], c_send.at[k, dy], c_recv.at[k, dy], s, core
        )

    def back_pair(k, dy):
        group = corner if dy else core
        return remote(
            part.at[k, group], rc.at[k, dy], rc_send.at[k, dy], rc_recv.at[k, dy], s, core
        )

    def back_plane(k):
        return remote(cs.at[k], ry.at[k], ry_send.at[k], ry_recv.at[k], s, plane_peer)

    def pass_hidden(k, r):
        to = flipped(t, r)
        return remote(
            hid.at[k, to], hidr.at[k, r], h_send.at[k, r - 1], h_recv.at[k, r - 1], s, to
        )

    def back(k):
        return remote(fin.at[k], ret.at[s], ra_send.at[k], ra_recv.at[k], flipped(s, k), t)

    def landed_tok(k, group, send, recv):
        remote(tok.at[k, group], tok.at[k, group], send, recv, s, core).wait_recv()

    order = step_order(sp)
    for k in order:
        if k:
            begin(arrive(k))
    tok[0, t] = outg[s]

    def spread(k):
        if k:
            landed_tok(k, t, a_send.at[k], a_recv.at[k])
        begin(plane(k))
        begin(pair(k, 0))

    def collect(k):
        landed_tok(k, plane_peer, y_send.at[k], y_recv.at[k])
        begin(pair(k, 1))
        landed_tok(k, core, c_send.at[k, 0], c_recv.at[k, 0])
        landed_tok(k, corner, c_send.at[k, 1], c_recv.at[k, 1])

    def compute(k):
        token_rows = tok[k].reshape(tp * cap, width)
        gated = jnp.dot(token_rows, gate[...], preferred_element_type=jnp.float32)
        upward = jnp.dot(token_rows, up[...], preferred_element_type=jnp.float32)
        hidden = (gated / (1.0 + jnp.exp(-gated)) * upward).astype(jnp.bfloat16)
        hid[k] = hidden.reshape(tp, cap, hidden.shape[1])
        hidr[k, 0] = hid[k, t]
        for r in range(1, tp):
            begin(pass_hidden(k, r))
        step = math.gcd(own_part, 512)

        @pl.loop(0, own_part // step)
        def _(n):
            start = pl.multiple_of(n * step, step)
            piece = jnp.dot(
                hidden,
                down[:, pl.ds(pl.multiple_of(shared + start, step), step)],
                preferred_element_type=jnp.float32,
            )
            part[k, :, :, pl.ds(start, step)] = piece.astype(jnp.bfloat16).reshape(tp, cap, step)

        for dy in (1, 0):
            begin(back_pair(k, dy))

    def reduce_pair(k):
        back_pair(k, 1).wait_recv()
        cs[k] = (
            part[k, plane_peer].astype(jnp.float32) + rc[k, 1].astype(jnp.float32)
        ).astype(jnp.bfloat16)
        begin(back_plane(k))

    def finish_steps(ks):
        for k in ks:
            for r in range(1, tp):
                pass_hidden(k, r).wait_recv()
        lefts = [jnp.concatenate([hidr[k, r] for k in ks], axis=0) for r in range(tp)]
        for n in range(chunks):
            columns = slice(n * chunk, (n + 1) * chunk)
            piece = jnp.dot(lefts[0], down[:, columns], preferred_element_type=jnp.float32)
            for r in range(1, tp):
                piece += jnp.dot(lefts[r], moved[n, r - 1], preferred_element_type=jnp.float32)
            piece = piece.astype(jnp.bfloat16)
            for i, k in enumerate(ks):
                fin[k, :, columns] = piece[i * cap:(i + 1) * cap]
        for k in ks:
            back_pair(k, 0).wait_recv()
            whole = part[k, t].astype(jnp.float32) + rc[k, 0].astype(jnp.float32)
            back_plane(k).wait_recv()
            whole = whole + ry[k].astype(jnp.float32)
            fin[k, :, shared:] = whole.astype(jnp.bfloat16)
            if k:
                begin(back(k))
            else:
                ret[s] = fin[k]

    lead = 2
    for k in order[:lead]:
        spread(k)
    for i, k in enumerate(order):
        if i == 0:
            for n in range(chunks):
                lend(n, 2).wait_recv()
                begin(relend(n))
        collect(k)
        if i == 0:
            for copy in fetches[8:10]:
                copy.wait()
        compute(k)
        if i == 1:
            for n in range(chunks):
                lend(n, 1).wait_recv()
                relend(n).wait_recv()
        if i % 2 and i > 1:
            finish_steps(order[i - 3:i - 1])
        reduce_pair(k)
        if i + lead < len(order):
            spread(order[i + lead])
    finish_steps(order[-2:])
    for k in range(1, sp):
        there = flipped(s, k)
        remote(ret.at[there], ret.at[there], ra_send.at[k], ra_recv.at[k], s, core).wait_recv()

    unit = lax.broadcasted_iota(jnp.int32, (sp * cap, sp * cap), 0) == lax.broadcasted_iota(
        jnp.int32, (sp * cap, sp * cap), 1
    )
    unit = jnp.where(unit, 1.0, 0.0).astype(jnp.bfloat16)

    def turned(table):
        return lax.dot_general(
            table, unit, (((0,), (0,)), ((), ())), preferred_element_type=jnp.float32
        ).astype(jnp.bfloat16)

    high = mix[...].astype(jnp.bfloat16)
    mix_low = turned((mix[...] - high.astype(jnp.float32)).astype(jnp.bfloat16))
    mix_high = turned(high)

    @pl.loop(0, width // tile)
    def _(n):
        columns = pl.ds(pl.multiple_of(n * tile, tile), tile)
        returned = ret[:, :, columns].reshape(sp * cap, tile)
        combined = jnp.dot(mix_high, returned, preferred_element_type=jnp.float32)
        combined += jnp.dot(mix_low, returned, preferred_element_type=jnp.float32)
        out[:, columns] = (normed[:, columns].astype(jnp.float32) + combined).astype(
            jnp.bfloat16
        )

    for copy in sends:
        copy.wait_send()
    for d in (2, 1):
        @pl.when(z + d < lanes)
        def _():
            along(s, s + 2 * d, d).wait_send()

    @pl.when(x == 0)
    def _():
        across(s, 0).wait_send()

    for level, order_of in ((1, (1,)), (2, (2, 1)), (3, (1, 2, 3))):
        @pl.when(z == level)
        def _():
            for d in order_of:
                if level + d == 4 and d == 2:
                    along(s - 2 * d, s + 2, 3).wait_send()
                across(s - 2 * d, d).wait_send()


def step_order(sp):
    far = [k for half in (3, 2) for k in (2 * half, 2 * half + 1)]
    return [0, 1, 2] + far + [3]


def layer(
    query_one, key_one, query_two, key_two, value, lambda_head, head_gain, out_weight,
    residual, norm_gain, route_expert, route_weight, gate, up, down,
):
    sp, tp = lax.axis_size("sp"), lax.axis_size("tp")
    local = query_one.shape[0]
    heads = lambda_head.shape[0]
    kv_heads = key_one.shape[1] // HEAD
    rows, width = residual.shape
    hidden = gate.shape[1]
    cap = slots(rows, route_expert.shape[1], sp)
    lanes, parts = sp // 2, 4
    chunk = width // 8
    chunks, early = CHUNKS, EARLY
    own_part = width - chunks * chunk
    vmem = pl.BlockSpec(memory_space=pltpu.VMEM)
    hbm = pl.BlockSpec(memory_space=pl.ANY)
    smem = pl.BlockSpec(memory_space=pltpu.SMEM)
    dma = pltpu.SemaphoreType.DMA
    bf16 = jnp.bfloat16
    return pl.pallas_call(
        functools.partial(layer_kernel, sp, tp, heads, kv_heads, cap, early),
        out_shape=jax.ShapeDtypeStruct((rows, width), bf16),
        in_specs=[hbm] * 5 + [smem, vmem, hbm, hbm] + [vmem] * 3 + [hbm] * 3,
        out_specs=vmem,
        scratch_shapes=[
            pltpu.VMEM(query_one.shape, bf16),
            pltpu.VMEM(query_two.shape, bf16),
            pltpu.VMEM(residual.shape, bf16),
            pltpu.VMEM((sp, local, 4 * kv_heads * HEAD), bf16),
            pltpu.VMEM(out_weight.shape, bf16),
            pltpu.VMEM((local, heads * 2 * HEAD), bf16),
            pltpu.VMEM((parts, tp, rows, width // parts), bf16),
            pltpu.VMEM((2, parts, rows, width // parts), bf16),
            pltpu.VMEM((parts, rows, width // parts), bf16),
            pltpu.VMEM((parts, rows, width // parts), bf16),
            pltpu.VMEM((rows, width), jnp.float32),
            pltpu.VMEM((rows, width), bf16),
            pltpu.VMEM((sp * cap, rows), bf16),
            pltpu.VMEM((sp * cap, rows), jnp.float32),
            pltpu.VMEM((width, hidden), bf16),
            pltpu.VMEM((width, hidden), bf16),
            pltpu.VMEM((hidden, width), bf16),
            pltpu.VMEM((chunks, tp - 1, hidden, chunk), bf16),
            pltpu.VMEM((sp, tp, cap, hidden), bf16),
            pltpu.VMEM((sp, tp, cap, hidden), bf16),
            pltpu.VMEM((sp, cap, width), bf16),
            pltpu.VMEM((sp, tp, cap, width), bf16),
            pltpu.VMEM((sp, tp, cap, own_part), bf16),
            pltpu.VMEM((sp, 2, cap, own_part), bf16),
            pltpu.VMEM((sp, cap, own_part), bf16),
            pltpu.VMEM((sp, cap, own_part), bf16),
            pltpu.VMEM((sp, cap, width), bf16),
            pltpu.VMEM((sp, cap, width), bf16),
            dma((10,)), dma((lanes,)), dma((lanes,)), dma((lanes,)), dma((lanes,)),
            dma((2, parts)), dma((2, parts)), dma((parts,)), dma((parts,)),
            dma((chunks, tp - 1)), dma((chunks, tp - 1)), dma((sp, tp - 1)), dma((sp, tp - 1)),
            dma((sp,)), dma((sp,)), dma((sp,)), dma((sp,)), dma((sp, 2)), dma((sp, 2)),
            dma((sp, 2)), dma((sp, 2)), dma((sp,)), dma((sp,)), dma((sp,)), dma((sp,)),
        ],
        compiler_params=pltpu.CompilerParams(
            collective_id=0, has_side_effects=True, vmem_limit_bytes=VMEM_BYTES
        ),
        name="layer",
    )(
        query_one, key_one, query_two, key_two, value, lambda_head,
        head_gain[None, :], out_weight, residual, norm_gain[None, :],
        route_expert.T, route_weight.T, gate, up, down,
    )


def on_device_kernels(*arrays):
    return layer(*arrays[:12], *(weight[0] for weight in arrays[12:]))


def slots(rows, top_count, experts):
    return max(2 * rows * top_count // experts, 2)


def fits(*arrays):
    query_one, residual, route_expert = arrays[0], arrays[8], arrays[10]
    sp, tp = lax.axis_size("sp"), lax.axis_size("tp")
    rows, top_count = route_expert.shape
    return (
        sp == 8
        and tp == 4
        and slots(rows, top_count, sp) % 16 == 0
        and rows % 16 == 0
        and query_one.shape[0] * sp <= 2048
        and residual.shape[1] % 1024 == 0
    )


def on_device(*arrays):
    if fits(*arrays):
        return on_device_kernels(*arrays)
    return on_device_collectives(*arrays)


def on_device_collectives(
    query_one,
    key_one,
    query_two,
    key_two,
    value,
    lambda_head,
    head_gain,
    out_weight,
    residual,
    norm_gain,
    route_expert,
    route_weight,
    expert_gate,
    expert_up,
    expert_down,
):
    local_tokens = query_one.shape[0]
    heads_here = lambda_head.shape[0]
    kv_here = key_one.shape[1] // HEAD
    per_key = heads_here // kv_here
    offset = lax.axis_index("sp") * local_tokens
    first_queries = query_one.reshape(local_tokens, kv_here, per_key, HEAD)
    second_queries = query_two.reshape(local_tokens, kv_here, per_key, HEAD)
    query_pos = offset + jnp.arange(local_tokens, dtype=jnp.int32)

    def initial():
        return (
            jnp.full((kv_here, per_key, local_tokens), -1e30, jnp.float32),
            jnp.zeros((kv_here, per_key, local_tokens), jnp.float32),
            jnp.zeros((local_tokens, kv_here, per_key, 2 * HEAD), jnp.float32),
        )

    carried = (initial(), initial())
    key_first = lax.all_gather(key_one, "sp", axis=0, tiled=True)
    key_second = lax.all_gather(key_two, "sp", axis=0, tiled=True)
    value_rows = lax.all_gather(value, "sp", axis=0, tiled=True)
    length = key_first.shape[0]
    key_width = math.gcd(length, 1024)

    def advance(block_index, carried):
        block_start = block_index * key_width

        def attend(carried):
            first_block = lax.dynamic_slice_in_dim(key_first, block_start, key_width, 0)
            second_block = lax.dynamic_slice_in_dim(key_second, block_start, key_width, 0)
            value_block = lax.dynamic_slice_in_dim(value_rows, block_start, key_width, 0)
            first_block = first_block.reshape(key_width, kv_here, HEAD)
            second_block = second_block.reshape(key_width, kv_here, HEAD)
            value_block = value_block.reshape(key_width, kv_here, 2 * HEAD)
            key_pos = block_start + jnp.arange(key_width, dtype=jnp.int32)
            allowed = key_pos[None, :] <= query_pos[:, None]
            return (
                map_step(carried[0], first_queries, first_block, value_block, allowed),
                map_step(carried[1], second_queries, second_block, value_block, allowed),
            )

        def unchanged(carried):
            return carried

        return lax.cond(block_start <= offset + local_tokens - 1, attend, unchanged, carried)

    state_one, state_two = lax.fori_loop(0, length // key_width, advance, carried)
    difference = finish(state_one) - lambda_head.reshape(kv_here, per_key)[
        None, :, :, None
    ] * finish(state_two)
    scaled = (
        difference
        * lax.rsqrt(jnp.mean(difference * difference, axis=-1, keepdims=True) + 1e-05)
        * head_gain
    )
    attended = scaled.astype(jnp.bfloat16).reshape(local_tokens, heads_here * 2 * HEAD)
    own_rows = residual.shape[0]
    projected = lax.psum_scatter(
        jnp.dot(attended, out_weight, preferred_element_type=jnp.float32).astype(jnp.bfloat16),
        "tp",
        scatter_dimension=0,
        tiled=True,
    ).astype(jnp.float32)
    summed_in = residual.astype(jnp.float32) + projected
    centered = summed_in - jnp.mean(summed_in, axis=-1, keepdims=True)
    variance = jnp.mean(centered * centered, axis=-1, keepdims=True)
    normed = (centered * lax.rsqrt(variance + 1e-05) * norm_gain).astype(jnp.bfloat16)
    experts = lax.axis_size("sp")
    tp_count = lax.axis_size("tp")
    model_width = normed.shape[1]
    top_count = route_expert.shape[1]
    capacity = max(2 * own_rows * top_count // experts, 2)
    chosen = route_expert.reshape(own_rows * top_count)
    onehot = (chosen[:, None] == jnp.arange(experts, dtype=jnp.int32)[None, :]).astype(jnp.int32)
    slot_index = jnp.sum((jnp.cumsum(onehot, axis=0) - onehot) * onehot, axis=1)
    target = chosen * capacity + slot_index
    placed = target[:, None] == jnp.arange(experts * capacity, dtype=jnp.int32)[None, :]
    placed = jnp.any(placed.reshape(own_rows, top_count, experts * capacity), axis=1).astype(
        jnp.bfloat16
    )
    outgoing = jnp.einsum("rp,rd->pd", placed, normed, preferred_element_type=jnp.float32)
    outgoing = outgoing.astype(jnp.bfloat16).reshape(experts, capacity, model_width)
    arrived = lax.all_to_all(outgoing, "sp", split_axis=0, concat_axis=0, tiled=True)
    all_rows = lax.all_gather(arrived, "tp", axis=0, tiled=True)
    token_rows = all_rows.reshape(-1, model_width)
    gated = jnp.dot(token_rows, expert_gate[0], preferred_element_type=jnp.float32)
    upward = jnp.dot(token_rows, expert_up[0], preferred_element_type=jnp.float32)
    hidden = (jax.nn.silu(gated) * upward).astype(jnp.bfloat16)
    partial_value = (
        jnp.dot(hidden, expert_down[0], preferred_element_type=jnp.float32)
        .astype(jnp.bfloat16)
        .reshape(tp_count, experts * capacity, model_width)
    )
    summed = (
        lax.psum_scatter(partial_value, "tp", scatter_dimension=0, tiled=True)
        .astype(jnp.float32)
        .reshape(experts, capacity, model_width)
    )
    returned = lax.all_to_all(
        summed.astype(jnp.bfloat16), "sp", split_axis=0, concat_axis=0, tiled=True
    )
    picked = returned.reshape(experts * capacity, model_width)[target]
    picked = picked.reshape(own_rows, top_count, model_width).astype(jnp.float32)
    combined = jnp.sum(route_weight[:, :, None] * picked, axis=1)
    return (normed.astype(jnp.float32) + combined).astype(jnp.bfloat16)


def solution(mesh):
    in_specs = (
        P("sp", "tp"),
        P("sp", "tp"),
        P("sp", "tp"),
        P("sp", "tp"),
        P("sp", "tp"),
        P("tp"),
        P(),
        P("tp", None),
        P(("sp", "tp"), None),
        P(),
        P(("sp", "tp"), None),
        P(("sp", "tp"), None),
        P("sp", None, "tp"),
        P("sp", None, "tp"),
        P("sp", "tp", None),
    )
    out_specs = P(("sp", "tp"), None)
    return jax.shard_map(
        on_device, mesh=mesh, in_specs=in_specs, out_specs=out_specs, check_vma=False
    )
```

```python
import functools
import math

import jax
import jax.numpy as jnp
from jax import lax
from jax.experimental import pallas as pl
from jax.experimental.pallas import tpu as pltpu
from jax.sharding import PartitionSpec as P

HEAD = 128
VMEM_BYTES = 58 * 1024 * 1024
CHUNKS, EARLY = 4, 3


def map_step(carried, query_rows, key_block, value_block, allowed):
    largest, totals, running = carried
    scores = jnp.einsum(
        "qcgd,kcd->cgqk", query_rows, key_block, preferred_element_type=jnp.float32
    ) * HEAD ** (-0.5)
    scores = jnp.where(allowed[None, None], scores, -jnp.inf)
    updated = jnp.maximum(largest, jnp.max(scores, axis=-1))
    weights = jnp.exp(scores - updated[..., None])
    rescale = jnp.exp(largest - updated)
    totals = totals * rescale + jnp.sum(weights, axis=-1)
    added = jnp.einsum(
        "cgqk,kce->qcge",
        weights.astype(jnp.bfloat16),
        value_block,
        preferred_element_type=jnp.float32,
    )
    running = running * jnp.transpose(rescale, (2, 0, 1))[..., None] + added
    return (updated, totals, running)


def finish(carried):
    return carried[2] / jnp.transpose(carried[1], (2, 0, 1))[..., None]


def remote(src, dst, send, recv, sp_to, tp_to):
    return pltpu.make_async_remote_copy(
        src_ref=src,
        dst_ref=dst,
        send_sem=send,
        recv_sem=recv,
        device_id={"sp": sp_to, "tp": tp_to},
        device_id_type=pl.DeviceIdType.MESH,
    )


def flipped(index, mask):
    bit = 1
    while bit <= mask:
        if mask & bit:
            index = index + bit - 2 * bit * lax.rem(lax.div(index, bit), 2)
        bit *= 2
    return index


def layer_kernel(
    sp, tp, heads, kv_heads, cap, early,
    q1_hbm, k1_hbm, q2_hbm, k2_hbm, v_hbm, lam, gain, ow_hbm, res_hbm, ngain,
    route_e, route_w, gate_hbm, up_hbm, down_hbm, out,
    q1, q2, res, kv, ow, att, pbuf, prc, pcs, pry, total, held_rows, placed, tables, mix,
    gate, up, down, moved, hid, hidr, outg, tok, part, rc, cs, ry, fin, ret,
    f_sem, z_send, z_recv, x_send, x_recv, pc_send, pc_recv, py_send, py_recv,
    t_send, t_recv, r_send, r_recv, d_send, d_recv, h_send, h_recv, a_send, a_recv, y_send, y_recv, c_send, c_recv,
    rc_send, rc_recv, ry_send, ry_recv, ra_send, ra_recv,
):
    s = lax.axis_index("sp")
    t = lax.axis_index("tp")
    z, x = lax.div(s, 2), lax.rem(s, 2)
    y, c = lax.div(t, 2), lax.rem(t, 2)
    lanes = sp // 2
    px = flipped(s, 1)
    core = flipped(t, 1)
    plane_peer = flipped(t, 2)
    corner = flipped(t, 3)
    local = q1.shape[0]
    rows, width = out.shape
    kw = kv_heads * HEAD
    chunks, chunk = moved.shape[0], moved.shape[3]
    shared = chunks * chunk
    own_part = width - shared

    barrier = pltpu.get_barrier_semaphore()
    peers = [(flipped(s, k), t) for k in range(1, sp)]
    peers += [(s, flipped(t, r)) for r in range(1, tp)]
    for sp_to, tp_to in peers:
        pl.semaphore_signal(
            barrier,
            inc=1,
            device_id={"sp": sp_to, "tp": tp_to},
            device_id_type=pl.DeviceIdType.MESH,
        )
    sources = [
        (k1_hbm, kv.at[s, :, 0:kw]), (k2_hbm, kv.at[s, :, kw:2 * kw]),
        (v_hbm, kv.at[s, :, 2 * kw:4 * kw]), (down_hbm, down), (q1_hbm, q1), (q2_hbm, q2),
        (ow_hbm, ow), (res_hbm, res), (gate_hbm, gate), (up_hbm, up),
    ]
    fetches = [
        pltpu.make_async_copy(src, dst, f_sem.at[i]) for i, (src, dst) in enumerate(sources)
    ]
    for copy in fetches:
        copy.start()
    for block in range(1, sp):
        @pl.when(block > s)
        def _():
            kv[block] = jnp.zeros(kv.shape[1:], kv.dtype)

    places = lax.broadcasted_iota(jnp.int32, (sp * cap, rows), 0).astype(jnp.float32)
    owner = jnp.floor((places + 0.5) / cap)
    slot = places - owner * cap
    named = jnp.zeros((sp * cap, rows), jnp.float32)
    share = jnp.zeros((sp * cap, rows), jnp.float32)
    for choice in range(route_e.shape[0]):
        match = route_e[choice:choice + 1, :].astype(jnp.float32) == owner
        named += jnp.where(match, 1.0, 0.0)
        share += jnp.where(match, route_w[choice:choice + 1, :], 0.0)
    earlier = lax.broadcasted_iota(jnp.int32, (rows, rows), 0) < lax.broadcasted_iota(
        jnp.int32, (rows, rows), 1
    )
    rank = jnp.dot(
        named.astype(jnp.bfloat16),
        jnp.where(earlier, 1.0, 0.0).astype(jnp.bfloat16),
        preferred_element_type=jnp.float32,
    )
    held = jnp.where(rank == slot, named, 0.0)
    placed[...] = held.astype(jnp.bfloat16).reshape(sp, cap, rows)
    mix[...] = share * held

    sends = []

    def begin(copy):
        copy.start()
        sends.append(copy)

    pieces = z_send.shape[1]
    span = local // pieces

    def along(block, to, d, i):
        part_of = kv.at[block, i * span:(i + 1) * span]
        return remote(part_of, part_of, z_send.at[d, i], z_recv.at[d, i], to, t)

    def across(block, d, i):
        part_of = kv.at[block, i * span:(i + 1) * span]
        return remote(part_of, part_of, x_send.at[d, i], x_recv.at[d, i], px, t)

    for copy in fetches[:3]:
        copy.wait()
    pl.semaphore_wait(barrier, len(peers))
    for d in (2, 1):
        @pl.when(z + d < lanes)
        def _():
            for i in range(pieces):
                along(s, s + 2 * d, d, i).start()

    @pl.when(x == 0)
    def _():
        for i in range(pieces):
            across(s, 0, i).start()

    def lend(n, r):
        to = flipped(t, r)
        columns = slice(n * chunk, (n + 1) * chunk)
        return remote(
            down.at[:, columns], moved.at[n, r - 1], d_send.at[n, r - 1], d_recv.at[n, r - 1],
            s, to,
        )

    def relend(n):
        return remote(
            moved.at[n, 1], moved.at[n, 2], d_send.at[n, 2], d_recv.at[n, 2], s, core
        )

    def table(j):
        there = flipped(s, 2 * j)
        pair_of = pl.ds(2 * lax.div(there, 2), 2)
        return remote(
            placed.at[pair_of], tables.at[j], t_send.at[j], t_recv.at[j], there, t
        )

    for j in range(1, lanes):
        begin(table(j))

    fetches[3].wait()
    for n in range(early):
        begin(lend(n, 2))
    for n in range(chunks):
        begin(lend(n, 1))

    for level, order in ((1, (1,)), (2, (2, 1)), (3, (1, 2, 3))):
        @pl.when(z == level)
        def _():
            for d in order:
                for i in range(pieces):
                    along(s - 2 * d, s, d, i).wait_recv()
                    if level + d == 4 and d == 2:
                        along(s - 2 * d, s + 2, 3, i).start()
                    across(s - 2 * d, d, i).start()
            for d in order:
                for i in range(pieces):
                    across(px - 2 * d, d, i).wait_recv()

    @pl.when(x == 1)
    def _():
        for i in range(pieces):
            across(px, 0, i).wait_recv()

    for copy in fetches[4:6]:
        copy.wait()
    length = sp * local
    key_pos = lax.broadcasted_iota(jnp.int32, (local, length), 1)
    query_pos = s * local + lax.broadcasted_iota(jnp.int32, (local, length), 0)
    allowed = key_pos <= query_pos
    per_key = heads // kv_heads
    for h in range(heads):
        g = h // per_key
        values = kv[:, :, 2 * kw + g * 2 * HEAD:2 * kw + (g + 1) * 2 * HEAD]
        values = values.reshape(length, 2 * HEAD)
        maps = []
        for which, q in ((0, q1), (1, q2)):
            start = which * kw + g * HEAD
            keys = kv[:, :, start:start + HEAD].reshape(length, HEAD)
            scores = lax.dot_general(
                q[:, h * HEAD:(h + 1) * HEAD],
                keys,
                (((1,), (1,)), ((), ())),
                preferred_element_type=jnp.float32,
            ) * HEAD ** (-0.5)
            scores = jnp.where(allowed, scores, -1e30)
            weights = jnp.exp(scores - jnp.max(scores, axis=-1, keepdims=True))
            totals = jnp.sum(weights, axis=-1, keepdims=True)
            added = jnp.dot(
                weights.astype(jnp.bfloat16), values, preferred_element_type=jnp.float32
            )
            maps.append(added / totals)
        difference = maps[0] - lam[h] * maps[1]
        scaled = (
            difference
            * lax.rsqrt(jnp.mean(difference * difference, axis=-1, keepdims=True) + 1e-05)
            * gain[...]
        )
        att[:, h * 2 * HEAD:(h + 1) * 2 * HEAD] = scaled.astype(jnp.bfloat16)

    fetches[6].wait()

    def share_pair(there, dy, p):
        group = flipped(core, 2) if dy else core
        return remote(
            pbuf.at[p, group], prc.at[dy, p], pc_send.at[dy, p], pc_recv.at[dy, p], s, core
        )

    def share_plane(p):
        return remote(pcs.at[p], pry.at[p], py_send.at[p], py_recv.at[p], s, plane_peer)

    parts = pbuf.shape[0]
    part_width = width // parts
    for p in range(parts + 1):
        if p < parts:
            piece = jnp.dot(
                att[...],
                ow[:, p * part_width:(p + 1) * part_width],
                preferred_element_type=jnp.float32,
            )
            pbuf[p] = piece.astype(jnp.bfloat16).reshape(tp, rows, part_width)
            for dy in (1, 0):
                begin(share_pair(None, dy, p))
        if p >= 1:
            share_pair(None, 1, p - 1).wait_recv()
            pcs[p - 1] = (
                pbuf[p - 1, plane_peer].astype(jnp.float32) + prc[1, p - 1].astype(jnp.float32)
            ).astype(jnp.bfloat16)
            begin(share_plane(p - 1))
    for n in range(early, chunks):
        begin(lend(n, 2))
    fetches[7].wait()
    summed = jnp.zeros((rows, 1), jnp.float32)
    for p in range(parts):
        columns = slice(p * part_width, (p + 1) * part_width)
        share_pair(None, 0, p).wait_recv()
        piece = pbuf[p, t].astype(jnp.float32) + prc[0, p].astype(jnp.float32)
        piece = piece + res[:, columns].astype(jnp.float32)
        share_plane(p).wait_recv()
        piece = piece + pry[p].astype(jnp.float32)
        total[:, columns] = piece
        summed += jnp.sum(piece, axis=-1, keepdims=True)
    centered = total[...] - summed / width
    variance = jnp.mean(centered * centered, axis=-1, keepdims=True)
    held_rows[0] = (centered * lax.rsqrt(variance + 1e-05) * ngain[...]).astype(jnp.bfloat16)

    tile = math.gcd(width, 1024)

    inner = (z > 0) & (z < lanes - 1)

    def to_row(j):
        return remote(
            held_rows.at[0], held_rows.at[j], r_send.at[j], r_recv.at[j], flipped(s, 2 * j), t
        )

    def pass_row():
        return remote(
            held_rows.at[2], held_rows.at[3], r_send.at[0], r_recv.at[3], flipped(s, 2), t
        )

    begin(to_row(1))
    begin(to_row(2))

    @pl.when(inner)
    def _():
        to_row(3).start()

    def arrive(j):
        k = 2 * j + 1
        return remote(outg.at[j], tok.at[k, t], a_send.at[k], a_recv.at[k], px, t)

    def select(j):
        if j:
            to_row(j).wait_recv()
        if j == 2:
            @pl.when(inner)
            def _():
                pass_row().start()
        if j:
            table(j).wait_recv()
            mine, other = tables[j, x], tables[j, 1 - x]
        else:
            mine, other = placed[s], placed[px]
        both = jnp.concatenate([mine, other], axis=0)
        for n in range(width // tile):
            columns = slice(n * tile, (n + 1) * tile)
            piece = jnp.dot(both, held_rows[j, :, columns], preferred_element_type=jnp.float32)
            piece = piece.astype(jnp.bfloat16)
            tok[2 * j, t, :, columns] = piece[:cap]
            outg[j, :, columns] = piece[cap:]
        begin(arrive(j))

    def plane(k):
        return remote(
            tok.at[k, t], tok.at[k, t], y_send.at[k], y_recv.at[k], s, plane_peer
        )

    def pair(k, dy):
        mine = plane_peer if dy else t
        return remote(
            tok.at[k, mine], tok.at[k, mine], c_send.at[k, dy], c_recv.at[k, dy], s, core
        )

    def back_pair(k, dy):
        group = corner if dy else core
        return remote(
            part.at[k, group], rc.at[k, dy], rc_send.at[k, dy], rc_recv.at[k, dy], s, core
        )

    def back_plane(k):
        return remote(cs.at[k], ry.at[k], ry_send.at[k], ry_recv.at[k], s, plane_peer)

    def pass_hidden(k, r):
        to = flipped(t, r)
        return remote(
            hid.at[k, to], hidr.at[k, r], h_send.at[k, r - 1], h_recv.at[k, r - 1], s, to
        )

    def back(k):
        return remote(fin.at[k], ret.at[s], ra_send.at[k], ra_recv.at[k], flipped(s, k), t)

    def landed_tok(k, group, send, recv):
        remote(tok.at[k, group], tok.at[k, group], send, recv, s, core).wait_recv()

    order = step_order(sp)

    def spread(k):
        if k % 2:
            landed_tok(k, t, a_send.at[k], a_recv.at[k])
        else:
            select(k // 2)
        begin(plane(k))
        begin(pair(k, 0))

    def relay(k):
        landed_tok(k, plane_peer, y_send.at[k], y_recv.at[k])
        begin(pair(k, 1))

    def collect(k):
        landed_tok(k, core, c_send.at[k, 0], c_recv.at[k, 0])
        landed_tok(k, corner, c_send.at[k, 1], c_recv.at[k, 1])

    def compute(k):
        token_rows = tok[k].reshape(tp * cap, width)
        gated = jnp.dot(token_rows, gate[...], preferred_element_type=jnp.float32)
        upward = jnp.dot(token_rows, up[...], preferred_element_type=jnp.float32)
        hidden = (gated / (1.0 + jnp.exp(-gated)) * upward).astype(jnp.bfloat16)
        hid[k] = hidden.reshape(tp, cap, hidden.shape[1])
        hidr[k, 0] = hid[k, t]
        for r in range(1, tp):
            begin(pass_hidden(k, r))
        step = math.gcd(own_part, 512)

        @pl.loop(0, own_part // step)
        def _(n):
            start = pl.multiple_of(n * step, step)
            piece = jnp.dot(
                hidden,
                down[:, pl.ds(pl.multiple_of(shared + start, step), step)],
                preferred_element_type=jnp.float32,
            )
            part[k, :, :, pl.ds(start, step)] = piece.astype(jnp.bfloat16).reshape(tp, cap, step)

        for dy in (1, 0):
            begin(back_pair(k, dy))

    def reduce_pair(k):
        back_pair(k, 1).wait_recv()
        cs[k] = (
            part[k, plane_peer].astype(jnp.float32) + rc[k, 1].astype(jnp.float32)
        ).astype(jnp.bfloat16)
        begin(back_plane(k))

    def finish_steps(ks):
        for k in ks:
            for r in range(1, tp):
                pass_hidden(k, r).wait_recv()
        lefts = [jnp.concatenate([hidr[k, r] for k in ks], axis=0) for r in range(tp)]
        for n in range(chunks):
            columns = slice(n * chunk, (n + 1) * chunk)
            piece = jnp.dot(lefts[0], down[:, columns], preferred_element_type=jnp.float32)
            for r in range(1, tp):
                piece += jnp.dot(lefts[r], moved[n, r - 1], preferred_element_type=jnp.float32)
            piece = piece.astype(jnp.bfloat16)
            for i, k in enumerate(ks):
                fin[k, :, columns] = piece[i * cap:(i + 1) * cap]
        for k in ks:
            back_pair(k, 0).wait_recv()
            whole = part[k, t].astype(jnp.float32) + rc[k, 0].astype(jnp.float32)
            back_plane(k).wait_recv()
            whole = whole + ry[k].astype(jnp.float32)
            fin[k, :, shared:] = whole.astype(jnp.bfloat16)
            if k:
                begin(back(k))
            else:
                ret[s] = fin[k]

    lead, lag = 3, 1
    for k in [0] + order[:lead - 1]:
        spread(k)
    relay(order[0])
    for n in range(chunks):
        lend(n, 2).wait_recv()
        begin(relend(n))
    for copy in fetches[8:10]:
        copy.wait()
    for i, k in enumerate(order):
        collect(k)
        compute(k)
        if i == 0:
            relay(0)
        if i + 1 < len(order) - 1:
            relay(order[i + 1])
        reduce_pair(k)
        if i + lead < len(order):
            spread(order[i + lead - 1])
        if i == lag:
            for n in range(chunks):
                lend(n, 1).wait_recv()
                relend(n).wait_recv()
        if i >= lag:
            finish_steps([order[i - lag]])
    for k in order[len(order) - lag:]:
        finish_steps([k])
    for k in range(1, sp):
        there = flipped(s, k)
        remote(ret.at[there], ret.at[there], ra_send.at[k], ra_recv.at[k], s, core).wait_recv()

    unit = lax.broadcasted_iota(jnp.int32, (sp * cap, sp * cap), 0) == lax.broadcasted_iota(
        jnp.int32, (sp * cap, sp * cap), 1
    )
    unit = jnp.where(unit, 1.0, 0.0).astype(jnp.bfloat16)

    def turned(table):
        return lax.dot_general(
            table, unit, (((0,), (0,)), ((), ())), preferred_element_type=jnp.float32
        ).astype(jnp.bfloat16)

    high = mix[...].astype(jnp.bfloat16)
    mix_low = turned((mix[...] - high.astype(jnp.float32)).astype(jnp.bfloat16))
    mix_high = turned(high)

    @pl.loop(0, width // tile)
    def _(n):
        columns = pl.ds(pl.multiple_of(n * tile, tile), tile)
        returned = ret[:, :, columns].reshape(sp * cap, tile)
        combined = jnp.dot(mix_high, returned, preferred_element_type=jnp.float32)
        combined += jnp.dot(mix_low, returned, preferred_element_type=jnp.float32)
        out[:, columns] = (held_rows[0, :, columns].astype(jnp.float32) + combined).astype(
            jnp.bfloat16
        )

    for copy in sends:
        copy.wait_send()

    @pl.when(inner)
    def _():
        to_row(3).wait_send()
        pass_row().wait_send()

    for i in range(pieces):
        for d in (2, 1):
            @pl.when(z + d < lanes)
            def _():
                along(s, s + 2 * d, d, i).wait_send()

        @pl.when(x == 0)
        def _():
            across(s, 0, i).wait_send()

        for level, order_of in ((1, (1,)), (2, (2, 1)), (3, (1, 2, 3))):
            @pl.when(z == level)
            def _():
                for d in order_of:
                    if level + d == 4 and d == 2:
                        along(s - 2 * d, s + 2, 3, i).wait_send()
                    across(s - 2 * d, d, i).wait_send()


def step_order(sp):
    far = [k for half in range(2, sp // 2) for k in (2 * half, 2 * half + 1)]
    return [1, 2] + far + [3, 0]


def layer(
    query_one, key_one, query_two, key_two, value, lambda_head, head_gain, out_weight,
    residual, norm_gain, route_expert, route_weight, gate, up, down,
):
    sp, tp = lax.axis_size("sp"), lax.axis_size("tp")
    local = query_one.shape[0]
    heads = lambda_head.shape[0]
    kv_heads = key_one.shape[1] // HEAD
    rows, width = residual.shape
    hidden = gate.shape[1]
    cap = slots(rows, route_expert.shape[1], sp)
    lanes, parts = sp // 2, 4
    chunk = width // 8
    chunks, early = CHUNKS, EARLY
    own_part = width - chunks * chunk
    vmem = pl.BlockSpec(memory_space=pltpu.VMEM)
    hbm = pl.BlockSpec(memory_space=pl.ANY)
    smem = pl.BlockSpec(memory_space=pltpu.SMEM)
    dma = pltpu.SemaphoreType.DMA
    bf16 = jnp.bfloat16
    return pl.pallas_call(
        functools.partial(layer_kernel, sp, tp, heads, kv_heads, cap, early),
        out_shape=jax.ShapeDtypeStruct((rows, width), bf16),
        in_specs=[hbm] * 5 + [smem, vmem, hbm, hbm] + [vmem] * 3 + [hbm] * 3,
        out_specs=vmem,
        scratch_shapes=[
            pltpu.VMEM(query_one.shape, bf16),
            pltpu.VMEM(query_two.shape, bf16),
            pltpu.VMEM(residual.shape, bf16),
            pltpu.VMEM((sp, local, 4 * kv_heads * HEAD), bf16),
            pltpu.VMEM(out_weight.shape, bf16),
            pltpu.VMEM((local, heads * 2 * HEAD), bf16),
            pltpu.VMEM((parts, tp, rows, width // parts), bf16),
            pltpu.VMEM((2, parts, rows, width // parts), bf16),
            pltpu.VMEM((parts, rows, width // parts), bf16),
            pltpu.VMEM((parts, rows, width // parts), bf16),
            pltpu.VMEM((rows, width), jnp.float32),
            pltpu.VMEM((lanes, rows, width), bf16),
            pltpu.VMEM((sp, cap, rows), bf16),
            pltpu.VMEM((lanes, 2, cap, rows), bf16),
            pltpu.VMEM((sp * cap, rows), jnp.float32),
            pltpu.VMEM((width, hidden), bf16),
            pltpu.VMEM((width, hidden), bf16),
            pltpu.VMEM((hidden, width), bf16),
            pltpu.VMEM((chunks, tp - 1, hidden, chunk), bf16),
            pltpu.VMEM((sp, tp, cap, hidden), bf16),
            pltpu.VMEM((sp, tp, cap, hidden), bf16),
            pltpu.VMEM((lanes, cap, width), bf16),
            pltpu.VMEM((sp, tp, cap, width), bf16),
            pltpu.VMEM((sp, tp, cap, own_part), bf16),
            pltpu.VMEM((sp, 2, cap, own_part), bf16),
            pltpu.VMEM((sp, cap, own_part), bf16),
            pltpu.VMEM((sp, cap, own_part), bf16),
            pltpu.VMEM((sp, cap, width), bf16),
            pltpu.VMEM((sp, cap, width), bf16),
            dma((10,)), dma((lanes, 2)), dma((lanes, 2)), dma((lanes, 2)), dma((lanes, 2)),
            dma((2, parts)), dma((2, parts)), dma((parts,)), dma((parts,)),
            dma((lanes,)), dma((lanes,)), dma((lanes,)), dma((lanes,)),
            dma((chunks, tp - 1)), dma((chunks, tp - 1)), dma((sp, tp - 1)), dma((sp, tp - 1)),
            dma((sp,)), dma((sp,)), dma((sp,)), dma((sp,)), dma((sp, 2)), dma((sp, 2)),
            dma((sp, 2)), dma((sp, 2)), dma((sp,)), dma((sp,)), dma((sp,)), dma((sp,)),
        ],
        compiler_params=pltpu.CompilerParams(
            collective_id=0, has_side_effects=True, vmem_limit_bytes=VMEM_BYTES
        ),
        name="layer",
    )(
        query_one, key_one, query_two, key_two, value, lambda_head,
        head_gain[None, :], out_weight, residual, norm_gain[None, :],
        route_expert.T, route_weight.T, gate, up, down,
    )


def on_device_kernels(*arrays):
    return layer(*arrays[:12], *(weight[0] for weight in arrays[12:]))


def slots(rows, top_count, experts):
    return max(2 * rows * top_count // experts, 2)


def fits(*arrays):
    query_one, residual, route_expert = arrays[0], arrays[8], arrays[10]
    sp, tp = lax.axis_size("sp"), lax.axis_size("tp")
    rows, top_count = route_expert.shape
    return (
        sp == 8
        and tp == 4
        and slots(rows, top_count, sp) % 16 == 0
        and rows % 16 == 0
        and query_one.shape[0] * sp <= 2048
        and residual.shape[1] % 1024 == 0
    )


def on_device(*arrays):
    if fits(*arrays):
        return on_device_kernels(*arrays)
    return on_device_collectives(*arrays)


def on_device_collectives(
    query_one,
    key_one,
    query_two,
    key_two,
    value,
    lambda_head,
    head_gain,
    out_weight,
    residual,
    norm_gain,
    route_expert,
    route_weight,
    expert_gate,
    expert_up,
    expert_down,
):
    local_tokens = query_one.shape[0]
    heads_here = lambda_head.shape[0]
    kv_here = key_one.shape[1] // HEAD
    per_key = heads_here // kv_here
    offset = lax.axis_index("sp") * local_tokens
    first_queries = query_one.reshape(local_tokens, kv_here, per_key, HEAD)
    second_queries = query_two.reshape(local_tokens, kv_here, per_key, HEAD)
    query_pos = offset + jnp.arange(local_tokens, dtype=jnp.int32)

    def initial():
        return (
            jnp.full((kv_here, per_key, local_tokens), -1e30, jnp.float32),
            jnp.zeros((kv_here, per_key, local_tokens), jnp.float32),
            jnp.zeros((local_tokens, kv_here, per_key, 2 * HEAD), jnp.float32),
        )

    carried = (initial(), initial())
    key_first = lax.all_gather(key_one, "sp", axis=0, tiled=True)
    key_second = lax.all_gather(key_two, "sp", axis=0, tiled=True)
    value_rows = lax.all_gather(value, "sp", axis=0, tiled=True)
    length = key_first.shape[0]
    key_width = math.gcd(length, 1024)

    def advance(block_index, carried):
        block_start = block_index * key_width

        def attend(carried):
            first_block = lax.dynamic_slice_in_dim(key_first, block_start, key_width, 0)
            second_block = lax.dynamic_slice_in_dim(key_second, block_start, key_width, 0)
            value_block = lax.dynamic_slice_in_dim(value_rows, block_start, key_width, 0)
            first_block = first_block.reshape(key_width, kv_here, HEAD)
            second_block = second_block.reshape(key_width, kv_here, HEAD)
            value_block = value_block.reshape(key_width, kv_here, 2 * HEAD)
            key_pos = block_start + jnp.arange(key_width, dtype=jnp.int32)
            allowed = key_pos[None, :] <= query_pos[:, None]
            return (
                map_step(carried[0], first_queries, first_block, value_block, allowed),
                map_step(carried[1], second_queries, second_block, value_block, allowed),
            )

        def unchanged(carried):
            return carried

        return lax.cond(block_start <= offset + local_tokens - 1, attend, unchanged, carried)

    state_one, state_two = lax.fori_loop(0, length // key_width, advance, carried)
    difference = finish(state_one) - lambda_head.reshape(kv_here, per_key)[
        None, :, :, None
    ] * finish(state_two)
    scaled = (
        difference
        * lax.rsqrt(jnp.mean(difference * difference, axis=-1, keepdims=True) + 1e-05)
        * head_gain
    )
    attended = scaled.astype(jnp.bfloat16).reshape(local_tokens, heads_here * 2 * HEAD)
    own_rows = residual.shape[0]
    projected = lax.psum_scatter(
        jnp.dot(attended, out_weight, preferred_element_type=jnp.float32).astype(jnp.bfloat16),
        "tp",
        scatter_dimension=0,
        tiled=True,
    ).astype(jnp.float32)
    summed_in = residual.astype(jnp.float32) + projected
    centered = summed_in - jnp.mean(summed_in, axis=-1, keepdims=True)
    variance = jnp.mean(centered * centered, axis=-1, keepdims=True)
    normed = (centered * lax.rsqrt(variance + 1e-05) * norm_gain).astype(jnp.bfloat16)
    experts = lax.axis_size("sp")
    tp_count = lax.axis_size("tp")
    model_width = normed.shape[1]
    top_count = route_expert.shape[1]
    capacity = max(2 * own_rows * top_count // experts, 2)
    chosen = route_expert.reshape(own_rows * top_count)
    onehot = (chosen[:, None] == jnp.arange(experts, dtype=jnp.int32)[None, :]).astype(jnp.int32)
    slot_index = jnp.sum((jnp.cumsum(onehot, axis=0) - onehot) * onehot, axis=1)
    target = chosen * capacity + slot_index
    placed = target[:, None] == jnp.arange(experts * capacity, dtype=jnp.int32)[None, :]
    placed = jnp.any(placed.reshape(own_rows, top_count, experts * capacity), axis=1).astype(
        jnp.bfloat16
    )
    outgoing = jnp.einsum("rp,rd->pd", placed, normed, preferred_element_type=jnp.float32)
    outgoing = outgoing.astype(jnp.bfloat16).reshape(experts, capacity, model_width)
    arrived = lax.all_to_all(outgoing, "sp", split_axis=0, concat_axis=0, tiled=True)
    all_rows = lax.all_gather(arrived, "tp", axis=0, tiled=True)
    token_rows = all_rows.reshape(-1, model_width)
    gated = jnp.dot(token_rows, expert_gate[0], preferred_element_type=jnp.float32)
    upward = jnp.dot(token_rows, expert_up[0], preferred_element_type=jnp.float32)
    hidden = (jax.nn.silu(gated) * upward).astype(jnp.bfloat16)
    partial_value = (
        jnp.dot(hidden, expert_down[0], preferred_element_type=jnp.float32)
        .astype(jnp.bfloat16)
        .reshape(tp_count, experts * capacity, model_width)
    )
    summed = (
        lax.psum_scatter(partial_value, "tp", scatter_dimension=0, tiled=True)
        .astype(jnp.float32)
        .reshape(experts, capacity, model_width)
    )
    returned = lax.all_to_all(
        summed.astype(jnp.bfloat16), "sp", split_axis=0, concat_axis=0, tiled=True
    )
    picked = returned.reshape(experts * capacity, model_width)[target]
    picked = picked.reshape(own_rows, top_count, model_width).astype(jnp.float32)
    combined = jnp.sum(route_weight[:, :, None] * picked, axis=1)
    return (normed.astype(jnp.float32) + combined).astype(jnp.bfloat16)


def solution(mesh):
    in_specs = (
        P("sp", "tp"),
        P("sp", "tp"),
        P("sp", "tp"),
        P("sp", "tp"),
        P("sp", "tp"),
        P("tp"),
        P(),
        P("tp", None),
        P(("sp", "tp"), None),
        P(),
        P(("sp", "tp"), None),
        P(("sp", "tp"), None),
        P("sp", None, "tp"),
        P("sp", None, "tp"),
        P("sp", "tp", None),
    )
    out_specs = P(("sp", "tp"), None)
    return jax.shard_map(
        on_device, mesh=mesh, in_specs=in_specs, out_specs=out_specs, check_vma=False
    )
```

```python
import functools
import math

import jax
import jax.numpy as jnp
from jax import lax
from jax.experimental import pallas as pl
from jax.experimental.pallas import tpu as pltpu
from jax.sharding import PartitionSpec as P

HEAD = 128
VMEM_BYTES = 58 * 1024 * 1024
CHUNKS, EARLY = 4, 3
PLAN = (
    "s0 s1 l0 s2", "r1 c1 s4 s3", "r2 w0 p1 c2", "s5 r4 f1 p2",
    "c4 s6 r5 f2", "p4 c5 s7 r6", "f4 p5 c6 r7", "f5 p6 r3 c7",
    "r0 f6 p7 c3", "f7 p3 c0 f3", "p0 f0",
)


def map_step(carried, query_rows, key_block, value_block, allowed):
    largest, totals, running = carried
    scores = jnp.einsum(
        "qcgd,kcd->cgqk", query_rows, key_block, preferred_element_type=jnp.float32
    ) * HEAD ** (-0.5)
    scores = jnp.where(allowed[None, None], scores, -jnp.inf)
    updated = jnp.maximum(largest, jnp.max(scores, axis=-1))
    weights = jnp.exp(scores - updated[..., None])
    rescale = jnp.exp(largest - updated)
    totals = totals * rescale + jnp.sum(weights, axis=-1)
    added = jnp.einsum(
        "cgqk,kce->qcge",
        weights.astype(jnp.bfloat16),
        value_block,
        preferred_element_type=jnp.float32,
    )
    running = running * jnp.transpose(rescale, (2, 0, 1))[..., None] + added
    return (updated, totals, running)


def finish(carried):
    return carried[2] / jnp.transpose(carried[1], (2, 0, 1))[..., None]


def remote(src, dst, send, recv, sp_to, tp_to):
    return pltpu.make_async_remote_copy(
        src_ref=src,
        dst_ref=dst,
        send_sem=send,
        recv_sem=recv,
        device_id={"sp": sp_to, "tp": tp_to},
        device_id_type=pl.DeviceIdType.MESH,
    )


def flipped(index, mask):
    bit = 1
    while bit <= mask:
        if mask & bit:
            index = index + bit - 2 * bit * lax.rem(lax.div(index, bit), 2)
        bit *= 2
    return index


def layer_kernel(
    sp, tp, heads, kv_heads, cap, early,
    q1_hbm, k1_hbm, q2_hbm, k2_hbm, v_hbm, lam, gain, ow_hbm, res_hbm, ngain,
    route_e, route_w, gate_hbm, up_hbm, down_hbm, out,
    q1, q2, res, kv, ow, att, pbuf, prc, pcs, pry, total, held_rows, placed, tables, mix,
    gate, up, down, moved, hid, hidr, outg, tok, part, rc, cs, ry, fin, ret,
    f_sem, z_send, z_recv, x_send, x_recv, pc_send, pc_recv, py_send, py_recv,
    t_send, t_recv, r_send, r_recv, d_send, d_recv, h_send, h_recv, a_send, a_recv, y_send, y_recv, c_send, c_recv,
    rc_send, rc_recv, ry_send, ry_recv, ra_send, ra_recv, result, o_sem,
):
    s = lax.axis_index("sp")
    t = lax.axis_index("tp")
    z, x = lax.div(s, 2), lax.rem(s, 2)
    y, c = lax.div(t, 2), lax.rem(t, 2)
    lanes = sp // 2
    px = flipped(s, 1)
    core = flipped(t, 1)
    plane_peer = flipped(t, 2)
    corner = flipped(t, 3)
    local = q1.shape[0]
    rows, width = out.shape
    kw = kv_heads * HEAD
    chunks, chunk = moved.shape[0], moved.shape[3]
    shared = chunks * chunk
    own_part = width - shared

    barrier = pltpu.get_barrier_semaphore()
    peers = [(flipped(s, k), t) for k in range(1, sp)]
    peers += [(s, flipped(t, r)) for r in range(1, tp)]
    for sp_to, tp_to in peers:
        pl.semaphore_signal(
            barrier,
            inc=1,
            device_id={"sp": sp_to, "tp": tp_to},
            device_id_type=pl.DeviceIdType.MESH,
        )
    sources = [
        (k1_hbm, kv.at[s, :, 0:kw]), (k2_hbm, kv.at[s, :, kw:2 * kw]),
        (v_hbm, kv.at[s, :, 2 * kw:4 * kw]), (down_hbm, down), (q1_hbm, q1), (q2_hbm, q2),
        (ow_hbm, ow), (res_hbm, res), (gate_hbm, gate), (up_hbm, up),
    ]
    fetches = [
        pltpu.make_async_copy(src, dst, f_sem.at[i]) for i, (src, dst) in enumerate(sources)
    ]
    for copy in fetches:
        copy.start()
    for block in range(1, sp):
        @pl.when(block > s)
        def _():
            kv[block] = jnp.zeros(kv.shape[1:], kv.dtype)

    places = lax.broadcasted_iota(jnp.int32, (sp * cap, rows), 0).astype(jnp.float32)
    owner = jnp.floor((places + 0.5) / cap)
    slot = places - owner * cap
    named = jnp.zeros((sp * cap, rows), jnp.float32)
    share = jnp.zeros((sp * cap, rows), jnp.float32)
    for choice in range(route_e.shape[0]):
        match = route_e[choice:choice + 1, :].astype(jnp.float32) == owner
        named += jnp.where(match, 1.0, 0.0)
        share += jnp.where(match, route_w[choice:choice + 1, :], 0.0)
    earlier = lax.broadcasted_iota(jnp.int32, (rows, rows), 0) < lax.broadcasted_iota(
        jnp.int32, (rows, rows), 1
    )
    rank = jnp.dot(
        named.astype(jnp.bfloat16),
        jnp.where(earlier, 1.0, 0.0).astype(jnp.bfloat16),
        preferred_element_type=jnp.float32,
    )
    held = jnp.where(rank == slot, named, 0.0)
    placed[...] = held.astype(jnp.bfloat16).reshape(sp, cap, rows)
    mix[...] = share * held

    sends = []

    def begin(copy):
        copy.start()
        sends.append(copy)

    pieces = z_send.shape[1]
    span = local // pieces

    def along(block, to, d, i):
        part_of = kv.at[block, i * span:(i + 1) * span]
        return remote(part_of, part_of, z_send.at[d, i], z_recv.at[d, i], to, t)

    def across(block, d, i):
        part_of = kv.at[block, i * span:(i + 1) * span]
        return remote(part_of, part_of, x_send.at[d, i], x_recv.at[d, i], px, t)

    for copy in fetches[:3]:
        copy.wait()
    pl.semaphore_wait(barrier, len(peers))
    for d in (2, 1):
        @pl.when(z + d < lanes)
        def _():
            for i in range(pieces):
                along(s, s + 2 * d, d, i).start()

    @pl.when(x == 0)
    def _():
        for i in range(pieces):
            across(s, 0, i).start()

    def lend(n, r):
        to = flipped(t, r)
        columns = slice(n * chunk, (n + 1) * chunk)
        return remote(
            down.at[:, columns], moved.at[n, r - 1], d_send.at[n, r - 1], d_recv.at[n, r - 1],
            s, to,
        )

    def relend(n):
        return remote(
            moved.at[n, 1], moved.at[n, 2], d_send.at[n, 2], d_recv.at[n, 2], s, core
        )

    def table(j):
        there = flipped(s, 2 * j)
        pair_of = pl.ds(2 * lax.div(there, 2), 2)
        return remote(
            placed.at[pair_of], tables.at[j], t_send.at[j], t_recv.at[j], there, t
        )

    for j in range(1, lanes):
        begin(table(j))

    fetches[3].wait()
    for n in range(early):
        begin(lend(n, 2))
    for n in range(chunks):
        begin(lend(n, 1))

    for level, order in ((1, (1,)), (2, (2, 1)), (3, (1, 2, 3))):
        @pl.when(z == level)
        def _():
            for d in order:
                for i in range(pieces):
                    along(s - 2 * d, s, d, i).wait_recv()
                    if level + d == 4 and d == 2:
                        along(s - 2 * d, s + 2, 3, i).start()
                    across(s - 2 * d, d, i).start()
            for d in order:
                for i in range(pieces):
                    across(px - 2 * d, d, i).wait_recv()

    @pl.when(x == 1)
    def _():
        for i in range(pieces):
            across(px, 0, i).wait_recv()

    for copy in fetches[4:6]:
        copy.wait()
    length = sp * local
    key_pos = lax.broadcasted_iota(jnp.int32, (local, length), 1)
    query_pos = s * local + lax.broadcasted_iota(jnp.int32, (local, length), 0)
    allowed = key_pos <= query_pos
    per_key = heads // kv_heads
    for h in range(heads):
        g = h // per_key
        values = kv[:, :, 2 * kw + g * 2 * HEAD:2 * kw + (g + 1) * 2 * HEAD]
        values = values.reshape(length, 2 * HEAD)
        maps = []
        for which, q in ((0, q1), (1, q2)):
            start = which * kw + g * HEAD
            keys = kv[:, :, start:start + HEAD].reshape(length, HEAD)
            scores = lax.dot_general(
                q[:, h * HEAD:(h + 1) * HEAD],
                keys,
                (((1,), (1,)), ((), ())),
                preferred_element_type=jnp.float32,
            ) * HEAD ** (-0.5)
            scores = jnp.where(allowed, scores, -1e30)
            weights = jnp.exp(scores - jnp.max(scores, axis=-1, keepdims=True))
            totals = jnp.sum(weights, axis=-1, keepdims=True)
            added = jnp.dot(
                weights.astype(jnp.bfloat16), values, preferred_element_type=jnp.float32
            )
            maps.append(added / totals)
        difference = maps[0] - lam[h] * maps[1]
        scaled = (
            difference
            * lax.rsqrt(jnp.mean(difference * difference, axis=-1, keepdims=True) + 1e-05)
            * gain[...]
        )
        att[:, h * 2 * HEAD:(h + 1) * 2 * HEAD] = scaled.astype(jnp.bfloat16)

    fetches[6].wait()

    def share_pair(there, dy, p):
        group = flipped(core, 2) if dy else core
        return remote(
            pbuf.at[p, group], prc.at[dy, p], pc_send.at[dy, p], pc_recv.at[dy, p], s, core
        )

    def share_plane(p):
        return remote(pcs.at[p], pry.at[p], py_send.at[p], py_recv.at[p], s, plane_peer)

    parts = pbuf.shape[0]
    part_width = width // parts
    for p in range(parts + 1):
        if p < parts:
            piece = jnp.dot(
                att[...],
                ow[:, p * part_width:(p + 1) * part_width],
                preferred_element_type=jnp.float32,
            )
            pbuf[p] = piece.astype(jnp.bfloat16).reshape(tp, rows, part_width)
            for dy in (1, 0):
                begin(share_pair(None, dy, p))
        if p >= 1:
            share_pair(None, 1, p - 1).wait_recv()
            pcs[p - 1] = (
                pbuf[p - 1, plane_peer].astype(jnp.float32) + prc[1, p - 1].astype(jnp.float32)
            ).astype(jnp.bfloat16)
            begin(share_plane(p - 1))
    for n in range(early, chunks):
        begin(lend(n, 2))
    fetches[7].wait()
    summed = jnp.zeros((rows, 1), jnp.float32)
    for p in range(parts):
        columns = slice(p * part_width, (p + 1) * part_width)
        share_pair(None, 0, p).wait_recv()
        piece = pbuf[p, t].astype(jnp.float32) + prc[0, p].astype(jnp.float32)
        piece = piece + res[:, columns].astype(jnp.float32)
        share_plane(p).wait_recv()
        piece = piece + pry[p].astype(jnp.float32)
        total[:, columns] = piece
        summed += jnp.sum(piece, axis=-1, keepdims=True)
    centered = total[...] - summed / width
    variance = jnp.mean(centered * centered, axis=-1, keepdims=True)
    held_rows[0] = (centered * lax.rsqrt(variance + 1e-05) * ngain[...]).astype(jnp.bfloat16)

    tile = math.gcd(width, 1024)

    inner = (z > 0) & (z < lanes - 1)

    def to_row(j):
        return remote(
            held_rows.at[0], held_rows.at[j], r_send.at[j], r_recv.at[j], flipped(s, 2 * j), t
        )

    def pass_row():
        return remote(
            held_rows.at[2], held_rows.at[3], r_send.at[0], r_recv.at[3], flipped(s, 2), t
        )

    begin(to_row(1))
    begin(to_row(2))

    @pl.when(inner)
    def _():
        to_row(3).start()

    def arrive(j):
        k = 2 * j + 1
        return remote(outg.at[j], tok.at[k, t], a_send.at[k], a_recv.at[k], px, t)

    def select(j):
        if j:
            to_row(j).wait_recv()
        if j == 2:
            @pl.when(inner)
            def _():
                pass_row().start()
        if j:
            table(j).wait_recv()
            mine, other = tables[j, x], tables[j, 1 - x]
        else:
            mine, other = placed[s], placed[px]
        both = jnp.concatenate([mine, other], axis=0)
        for n in range(width // tile):
            columns = slice(n * tile, (n + 1) * tile)
            piece = jnp.dot(both, held_rows[j, :, columns], preferred_element_type=jnp.float32)
            piece = piece.astype(jnp.bfloat16)
            tok[2 * j, t, :, columns] = piece[:cap]
            outg[j, :, columns] = piece[cap:]
        begin(arrive(j))

    def plane(k):
        return remote(
            tok.at[k, t], tok.at[k, t], y_send.at[k], y_recv.at[k], s, plane_peer
        )

    def pair(k, dy):
        mine = plane_peer if dy else t
        return remote(
            tok.at[k, mine], tok.at[k, mine], c_send.at[k, dy], c_recv.at[k, dy], s, core
        )

    def back_pair(k, dy):
        group = corner if dy else core
        return remote(
            part.at[k, group], rc.at[k, dy], rc_send.at[k, dy], rc_recv.at[k, dy], s, core
        )

    def back_plane(k):
        return remote(cs.at[k], ry.at[k], ry_send.at[k], ry_recv.at[k], s, plane_peer)

    def pass_hidden(k, r):
        to = flipped(t, r)
        return remote(
            hid.at[k, to], hidr.at[k, r], h_send.at[k, r - 1], h_recv.at[k, r - 1], s, to
        )

    def back(k):
        return remote(fin.at[k], ret.at[s], ra_send.at[k], ra_recv.at[k], flipped(s, k), t)

    def landed_tok(k, group, send, recv):
        remote(tok.at[k, group], tok.at[k, group], send, recv, s, core).wait_recv()

    def spread(k):
        if k % 2:
            landed_tok(k, t, a_send.at[k], a_recv.at[k])
        else:
            select(k // 2)
        begin(plane(k))
        begin(pair(k, 0))

    def relay(k):
        landed_tok(k, plane_peer, y_send.at[k], y_recv.at[k])
        begin(pair(k, 1))

    def collect(k):
        landed_tok(k, core, c_send.at[k, 0], c_recv.at[k, 0])
        landed_tok(k, corner, c_send.at[k, 1], c_recv.at[k, 1])

    def compute(k):
        token_rows = tok[k].reshape(tp * cap, width)
        gated = jnp.dot(token_rows, gate[...], preferred_element_type=jnp.float32)
        upward = jnp.dot(token_rows, up[...], preferred_element_type=jnp.float32)
        hidden = (gated / (1.0 + jnp.exp(-gated)) * upward).astype(jnp.bfloat16)
        hid[k] = hidden.reshape(tp, cap, hidden.shape[1])
        hidr[k, 0] = hid[k, t]
        for r in range(1, tp):
            begin(pass_hidden(k, r))
        step = math.gcd(own_part, 512)

        @pl.loop(0, own_part // step)
        def _(n):
            start = pl.multiple_of(n * step, step)
            piece = jnp.dot(
                hidden,
                down[:, pl.ds(pl.multiple_of(shared + start, step), step)],
                preferred_element_type=jnp.float32,
            )
            part[k, :, :, pl.ds(start, step)] = piece.astype(jnp.bfloat16).reshape(tp, cap, step)

        for dy in (1, 0):
            begin(back_pair(k, dy))

    def reduce_pair(k):
        back_pair(k, 1).wait_recv()
        cs[k] = (
            part[k, plane_peer].astype(jnp.float32) + rc[k, 1].astype(jnp.float32)
        ).astype(jnp.bfloat16)
        begin(back_plane(k))

    def finish_steps(ks):
        for k in ks:
            for r in range(1, tp):
                pass_hidden(k, r).wait_recv()
        lefts = [jnp.concatenate([hidr[k, r] for k in ks], axis=0) for r in range(tp)]
        for n in range(chunks):
            columns = slice(n * chunk, (n + 1) * chunk)
            piece = jnp.dot(lefts[0], down[:, columns], preferred_element_type=jnp.float32)
            for r in range(1, tp):
                piece += jnp.dot(lefts[r], moved[n, r - 1], preferred_element_type=jnp.float32)
            piece = piece.astype(jnp.bfloat16)
            for i, k in enumerate(ks):
                fin[k, :, columns] = piece[i * cap:(i + 1) * cap]
        for k in ks:
            back_pair(k, 0).wait_recv()
            whole = part[k, t].astype(jnp.float32) + rc[k, 0].astype(jnp.float32)
            back_plane(k).wait_recv()
            whole = whole + ry[k].astype(jnp.float32)
            fin[k, :, shared:] = whole.astype(jnp.bfloat16)
            if k:
                begin(back(k))
            else:
                ret[s] = fin[k]

    def begin_lent(_):
        for n in range(chunks):
            lend(n, 2).wait_recv()
            begin(relend(n))
        for copy in fetches[8:10]:
            copy.wait()

    def wait_lent(_):
        for n in range(chunks):
            lend(n, 1).wait_recv()
            relend(n).wait_recv()

    actions = {
        "s": [spread], "r": [relay], "c": [collect, compute], "p": [reduce_pair],
        "f": [lambda k: finish_steps([k])], "l": [begin_lent], "w": [wait_lent],
    }
    for action in " ".join(PLAN).split():
        for part_of in actions[action[0]]:
            part_of(int(action[1]))
    for k in range(1, sp):
        there = flipped(s, k)
        remote(ret.at[there], ret.at[there], ra_send.at[k], ra_recv.at[k], s, core).wait_recv()

    unit = lax.broadcasted_iota(jnp.int32, (sp * cap, sp * cap), 0) == lax.broadcasted_iota(
        jnp.int32, (sp * cap, sp * cap), 1
    )
    unit = jnp.where(unit, 1.0, 0.0).astype(jnp.bfloat16)

    def turned(table):
        return lax.dot_general(
            table, unit, (((0,), (0,)), ((), ())), preferred_element_type=jnp.float32
        ).astype(jnp.bfloat16)

    high = mix[...].astype(jnp.bfloat16)
    mix_low = turned((mix[...] - high.astype(jnp.float32)).astype(jnp.bfloat16))
    mix_high = turned(high)

    leaving = []
    for n in range(width // tile):
        columns = slice(n * tile, (n + 1) * tile)
        returned = ret[:, :, columns].reshape(sp * cap, tile)
        combined = jnp.dot(mix_high, returned, preferred_element_type=jnp.float32)
        combined += jnp.dot(mix_low, returned, preferred_element_type=jnp.float32)
        result[:, columns] = (held_rows[0, :, columns].astype(jnp.float32) + combined).astype(
            jnp.bfloat16
        )
        leaving.append(
            pltpu.make_async_copy(result.at[:, columns], out.at[:, columns], o_sem.at[n])
        )
        leaving[-1].start()

    for copy in sends:
        copy.wait_send()

    @pl.when(inner)
    def _():
        to_row(3).wait_send()
        pass_row().wait_send()

    for i in range(pieces):
        for d in (2, 1):
            @pl.when(z + d < lanes)
            def _():
                along(s, s + 2 * d, d, i).wait_send()

        @pl.when(x == 0)
        def _():
            across(s, 0, i).wait_send()

        for level, order_of in ((1, (1,)), (2, (2, 1)), (3, (1, 2, 3))):
            @pl.when(z == level)
            def _():
                for d in order_of:
                    if level + d == 4 and d == 2:
                        along(s - 2 * d, s + 2, 3, i).wait_send()
                    across(s - 2 * d, d, i).wait_send()

    for copy in leaving:
        copy.wait()


def layer(
    query_one, key_one, query_two, key_two, value, lambda_head, head_gain, out_weight,
    residual, norm_gain, route_expert, route_weight, gate, up, down,
):
    sp, tp = lax.axis_size("sp"), lax.axis_size("tp")
    local = query_one.shape[0]
    heads = lambda_head.shape[0]
    kv_heads = key_one.shape[1] // HEAD
    rows, width = residual.shape
    hidden = gate.shape[1]
    cap = slots(rows, route_expert.shape[1], sp)
    lanes, parts = sp // 2, 4
    chunk = width // 8
    chunks, early = CHUNKS, EARLY
    own_part = width - chunks * chunk
    vmem = pl.BlockSpec(memory_space=pltpu.VMEM)
    hbm = pl.BlockSpec(memory_space=pl.ANY)
    smem = pl.BlockSpec(memory_space=pltpu.SMEM)
    dma = pltpu.SemaphoreType.DMA
    bf16 = jnp.bfloat16
    return pl.pallas_call(
        functools.partial(layer_kernel, sp, tp, heads, kv_heads, cap, early),
        out_shape=jax.ShapeDtypeStruct((rows, width), bf16),
        in_specs=[hbm] * 5 + [smem, vmem, hbm, hbm] + [vmem] * 3 + [hbm] * 3,
        out_specs=hbm,
        scratch_shapes=[
            pltpu.VMEM(query_one.shape, bf16),
            pltpu.VMEM(query_two.shape, bf16),
            pltpu.VMEM(residual.shape, bf16),
            pltpu.VMEM((sp, local, 4 * kv_heads * HEAD), bf16),
            pltpu.VMEM(out_weight.shape, bf16),
            pltpu.VMEM((local, heads * 2 * HEAD), bf16),
            pltpu.VMEM((parts, tp, rows, width // parts), bf16),
            pltpu.VMEM((2, parts, rows, width // parts), bf16),
            pltpu.VMEM((parts, rows, width // parts), bf16),
            pltpu.VMEM((parts, rows, width // parts), bf16),
            pltpu.VMEM((rows, width), jnp.float32),
            pltpu.VMEM((lanes, rows, width), bf16),
            pltpu.VMEM((sp, cap, rows), bf16),
            pltpu.VMEM((lanes, 2, cap, rows), bf16),
            pltpu.VMEM((sp * cap, rows), jnp.float32),
            pltpu.VMEM((width, hidden), bf16),
            pltpu.VMEM((width, hidden), bf16),
            pltpu.VMEM((hidden, width), bf16),
            pltpu.VMEM((chunks, tp - 1, hidden, chunk), bf16),
            pltpu.VMEM((sp, tp, cap, hidden), bf16),
            pltpu.VMEM((sp, tp, cap, hidden), bf16),
            pltpu.VMEM((lanes, cap, width), bf16),
            pltpu.VMEM((sp, tp, cap, width), bf16),
            pltpu.VMEM((sp, tp, cap, own_part), bf16),
            pltpu.VMEM((sp, 2, cap, own_part), bf16),
            pltpu.VMEM((sp, cap, own_part), bf16),
            pltpu.VMEM((sp, cap, own_part), bf16),
            pltpu.VMEM((sp, cap, width), bf16),
            pltpu.VMEM((sp, cap, width), bf16),
            dma((10,)), dma((lanes, 4)), dma((lanes, 4)), dma((lanes, 4)), dma((lanes, 4)),
            dma((2, parts)), dma((2, parts)), dma((parts,)), dma((parts,)),
            dma((lanes,)), dma((lanes,)), dma((lanes,)), dma((lanes,)),
            dma((chunks, tp - 1)), dma((chunks, tp - 1)), dma((sp, tp - 1)), dma((sp, tp - 1)),
            dma((sp,)), dma((sp,)), dma((sp,)), dma((sp,)), dma((sp, 2)), dma((sp, 2)),
            dma((sp, 2)), dma((sp, 2)), dma((sp,)), dma((sp,)), dma((sp,)), dma((sp,)),
            pltpu.VMEM((rows, width), bf16), dma((width // math.gcd(width, 1024),)),
        ],
        compiler_params=pltpu.CompilerParams(
            collective_id=0, has_side_effects=True, vmem_limit_bytes=VMEM_BYTES
        ),
        name="layer",
    )(
        query_one, key_one, query_two, key_two, value, lambda_head,
        head_gain[None, :], out_weight, residual, norm_gain[None, :],
        route_expert.T, route_weight.T, gate, up, down,
    )


def on_device_kernels(*arrays):
    return layer(*arrays[:12], *(weight[0] for weight in arrays[12:]))


def slots(rows, top_count, experts):
    return max(2 * rows * top_count // experts, 2)


def fits(*arrays):
    query_one, residual, route_expert = arrays[0], arrays[8], arrays[10]
    sp, tp = lax.axis_size("sp"), lax.axis_size("tp")
    rows, top_count = route_expert.shape
    return (
        sp == 8
        and tp == 4
        and slots(rows, top_count, sp) % 16 == 0
        and rows % 16 == 0
        and query_one.shape[0] * sp <= 2048
        and residual.shape[1] % 1024 == 0
    )


def on_device(*arrays):
    if fits(*arrays):
        return on_device_kernels(*arrays)
    return on_device_collectives(*arrays)


def on_device_collectives(
    query_one,
    key_one,
    query_two,
    key_two,
    value,
    lambda_head,
    head_gain,
    out_weight,
    residual,
    norm_gain,
    route_expert,
    route_weight,
    expert_gate,
    expert_up,
    expert_down,
):
    local_tokens = query_one.shape[0]
    heads_here = lambda_head.shape[0]
    kv_here = key_one.shape[1] // HEAD
    per_key = heads_here // kv_here
    offset = lax.axis_index("sp") * local_tokens
    first_queries = query_one.reshape(local_tokens, kv_here, per_key, HEAD)
    second_queries = query_two.reshape(local_tokens, kv_here, per_key, HEAD)
    query_pos = offset + jnp.arange(local_tokens, dtype=jnp.int32)

    def initial():
        return (
            jnp.full((kv_here, per_key, local_tokens), -1e30, jnp.float32),
            jnp.zeros((kv_here, per_key, local_tokens), jnp.float32),
            jnp.zeros((local_tokens, kv_here, per_key, 2 * HEAD), jnp.float32),
        )

    carried = (initial(), initial())
    key_first = lax.all_gather(key_one, "sp", axis=0, tiled=True)
    key_second = lax.all_gather(key_two, "sp", axis=0, tiled=True)
    value_rows = lax.all_gather(value, "sp", axis=0, tiled=True)
    length = key_first.shape[0]
    key_width = math.gcd(length, 1024)

    def advance(block_index, carried):
        block_start = block_index * key_width

        def attend(carried):
            first_block = lax.dynamic_slice_in_dim(key_first, block_start, key_width, 0)
            second_block = lax.dynamic_slice_in_dim(key_second, block_start, key_width, 0)
            value_block = lax.dynamic_slice_in_dim(value_rows, block_start, key_width, 0)
            first_block = first_block.reshape(key_width, kv_here, HEAD)
            second_block = second_block.reshape(key_width, kv_here, HEAD)
            value_block = value_block.reshape(key_width, kv_here, 2 * HEAD)
            key_pos = block_start + jnp.arange(key_width, dtype=jnp.int32)
            allowed = key_pos[None, :] <= query_pos[:, None]
            return (
                map_step(carried[0], first_queries, first_block, value_block, allowed),
                map_step(carried[1], second_queries, second_block, value_block, allowed),
            )

        def unchanged(carried):
            return carried

        return lax.cond(block_start <= offset + local_tokens - 1, attend, unchanged, carried)

    state_one, state_two = lax.fori_loop(0, length // key_width, advance, carried)
    difference = finish(state_one) - lambda_head.reshape(kv_here, per_key)[
        None, :, :, None
    ] * finish(state_two)
    scaled = (
        difference
        * lax.rsqrt(jnp.mean(difference * difference, axis=-1, keepdims=True) + 1e-05)
        * head_gain
    )
    attended = scaled.astype(jnp.bfloat16).reshape(local_tokens, heads_here * 2 * HEAD)
    own_rows = residual.shape[0]
    projected = lax.psum_scatter(
        jnp.dot(attended, out_weight, preferred_element_type=jnp.float32).astype(jnp.bfloat16),
        "tp",
        scatter_dimension=0,
        tiled=True,
    ).astype(jnp.float32)
    summed_in = residual.astype(jnp.float32) + projected
    centered = summed_in - jnp.mean(summed_in, axis=-1, keepdims=True)
    variance = jnp.mean(centered * centered, axis=-1, keepdims=True)
    normed = (centered * lax.rsqrt(variance + 1e-05) * norm_gain).astype(jnp.bfloat16)
    experts = lax.axis_size("sp")
    tp_count = lax.axis_size("tp")
    model_width = normed.shape[1]
    top_count = route_expert.shape[1]
    capacity = max(2 * own_rows * top_count // experts, 2)
    chosen = route_expert.reshape(own_rows * top_count)
    onehot = (chosen[:, None] == jnp.arange(experts, dtype=jnp.int32)[None, :]).astype(jnp.int32)
    slot_index = jnp.sum((jnp.cumsum(onehot, axis=0) - onehot) * onehot, axis=1)
    target = chosen * capacity + slot_index
    placed = target[:, None] == jnp.arange(experts * capacity, dtype=jnp.int32)[None, :]
    placed = jnp.any(placed.reshape(own_rows, top_count, experts * capacity), axis=1).astype(
        jnp.bfloat16
    )
    outgoing = jnp.einsum("rp,rd->pd", placed, normed, preferred_element_type=jnp.float32)
    outgoing = outgoing.astype(jnp.bfloat16).reshape(experts, capacity, model_width)
    arrived = lax.all_to_all(outgoing, "sp", split_axis=0, concat_axis=0, tiled=True)
    all_rows = lax.all_gather(arrived, "tp", axis=0, tiled=True)
    token_rows = all_rows.reshape(-1, model_width)
    gated = jnp.dot(token_rows, expert_gate[0], preferred_element_type=jnp.float32)
    upward = jnp.dot(token_rows, expert_up[0], preferred_element_type=jnp.float32)
    hidden = (jax.nn.silu(gated) * upward).astype(jnp.bfloat16)
    partial_value = (
        jnp.dot(hidden, expert_down[0], preferred_element_type=jnp.float32)
        .astype(jnp.bfloat16)
        .reshape(tp_count, experts * capacity, model_width)
    )
    summed = (
        lax.psum_scatter(partial_value, "tp", scatter_dimension=0, tiled=True)
        .astype(jnp.float32)
        .reshape(experts, capacity, model_width)
    )
    returned = lax.all_to_all(
        summed.astype(jnp.bfloat16), "sp", split_axis=0, concat_axis=0, tiled=True
    )
    picked = returned.reshape(experts * capacity, model_width)[target]
    picked = picked.reshape(own_rows, top_count, model_width).astype(jnp.float32)
    combined = jnp.sum(route_weight[:, :, None] * picked, axis=1)
    return (normed.astype(jnp.float32) + combined).astype(jnp.bfloat16)


def solution(mesh):
    in_specs = (
        P("sp", "tp"),
        P("sp", "tp"),
        P("sp", "tp"),
        P("sp", "tp"),
        P("sp", "tp"),
        P("tp"),
        P(),
        P("tp", None),
        P(("sp", "tp"), None),
        P(),
        P(("sp", "tp"), None),
        P(("sp", "tp"), None),
        P("sp", None, "tp"),
        P("sp", None, "tp"),
        P("sp", "tp", None),
    )
    out_specs = P(("sp", "tp"), None)
    return jax.shard_map(
        on_device, mesh=mesh, in_specs=in_specs, out_specs=out_specs, check_vma=False
    )
```

```python
import functools
import math

import jax
import jax.numpy as jnp
from jax import lax
from jax.experimental import pallas as pl
from jax.experimental.pallas import tpu as pltpu
from jax.sharding import PartitionSpec as P

HEAD = 128
VMEM_BYTES = 58 * 1024 * 1024
CHUNKS, EARLY = 4, 3
PLAN = (
    "s0 s1 l0 s2", "r1 c1 s4 s3", "r2 w0 p1 c2", "s5 h1 r4 p2",
    "f1 c4 h2 s6", "r5 p4 f2 c5", "h4 s7 r6 p5", "f4 c6 h5 r7",
    "p6 f5 r3 c7", "h6 r0 p7 f6", "c3 h7 p3 f7", "c0 h3 p0 f3",
    "h0 f0",
)


def map_step(carried, query_rows, key_block, value_block, allowed):
    largest, totals, running = carried
    scores = jnp.einsum(
        "qcgd,kcd->cgqk", query_rows, key_block, preferred_element_type=jnp.float32
    ) * HEAD ** (-0.5)
    scores = jnp.where(allowed[None, None], scores, -jnp.inf)
    updated = jnp.maximum(largest, jnp.max(scores, axis=-1))
    weights = jnp.exp(scores - updated[..., None])
    rescale = jnp.exp(largest - updated)
    totals = totals * rescale + jnp.sum(weights, axis=-1)
    added = jnp.einsum(
        "cgqk,kce->qcge",
        weights.astype(jnp.bfloat16),
        value_block,
        preferred_element_type=jnp.float32,
    )
    running = running * jnp.transpose(rescale, (2, 0, 1))[..., None] + added
    return (updated, totals, running)


def finish(carried):
    return carried[2] / jnp.transpose(carried[1], (2, 0, 1))[..., None]


def remote(src, dst, send, recv, sp_to, tp_to):
    return pltpu.make_async_remote_copy(
        src_ref=src,
        dst_ref=dst,
        send_sem=send,
        recv_sem=recv,
        device_id={"sp": sp_to, "tp": tp_to},
        device_id_type=pl.DeviceIdType.MESH,
    )


def flipped(index, mask):
    bit = 1
    while bit <= mask:
        if mask & bit:
            index = index + bit - 2 * bit * lax.rem(lax.div(index, bit), 2)
        bit *= 2
    return index


def layer_kernel(
    sp, tp, heads, kv_heads, cap, early,
    q1_hbm, k1_hbm, q2_hbm, k2_hbm, v_hbm, lam, gain, ow_hbm, res_hbm, ngain,
    route_e, route_w, gate_hbm, up_hbm, down_hbm, out,
    q1, q2, res, kv, ow, att, pbuf, prc, pcs, pry, total, held_rows, placed, tables, mix,
    gate, up, down, moved, hid, hidr, outg, tok, part, rc, cs, ry, fin, ret,
    f_sem, z_send, z_recv, x_send, x_recv, pc_send, pc_recv, py_send, py_recv,
    t_send, t_recv, r_send, r_recv, d_send, d_recv, h_send, h_recv, a_send, a_recv, y_send, y_recv, c_send, c_recv,
    rc_send, rc_recv, ry_send, ry_recv, ra_send, ra_recv, result, o_sem,
):
    s = lax.axis_index("sp")
    t = lax.axis_index("tp")
    z, x = lax.div(s, 2), lax.rem(s, 2)
    y, c = lax.div(t, 2), lax.rem(t, 2)
    lanes = sp // 2
    px = flipped(s, 1)
    core = flipped(t, 1)
    plane_peer = flipped(t, 2)
    corner = flipped(t, 3)
    local = q1.shape[0]
    rows, width = out.shape
    kw = kv_heads * HEAD
    chunks, chunk = moved.shape[0], moved.shape[3]
    shared = chunks * chunk
    own_part = width - shared

    barrier = pltpu.get_barrier_semaphore()
    peers = [(flipped(s, k), t) for k in range(1, sp)]
    peers += [(s, flipped(t, r)) for r in range(1, tp)]
    for sp_to, tp_to in peers:
        pl.semaphore_signal(
            barrier,
            inc=1,
            device_id={"sp": sp_to, "tp": tp_to},
            device_id_type=pl.DeviceIdType.MESH,
        )
    sources = [
        (k1_hbm, kv.at[s, :, 0:kw]), (k2_hbm, kv.at[s, :, kw:2 * kw]),
        (v_hbm, kv.at[s, :, 2 * kw:4 * kw]), (down_hbm, down), (q1_hbm, q1), (q2_hbm, q2),
        (ow_hbm, ow), (res_hbm, res), (gate_hbm, gate), (up_hbm, up),
    ]
    fetches = [
        pltpu.make_async_copy(src, dst, f_sem.at[i]) for i, (src, dst) in enumerate(sources)
    ]
    for copy in fetches:
        copy.start()
    for block in range(1, sp):
        @pl.when(block > s)
        def _():
            kv[block] = jnp.zeros(kv.shape[1:], kv.dtype)

    places = lax.broadcasted_iota(jnp.int32, (sp * cap, rows), 0).astype(jnp.float32)
    owner = jnp.floor((places + 0.5) / cap)
    slot = places - owner * cap
    named = jnp.zeros((sp * cap, rows), jnp.float32)
    share = jnp.zeros((sp * cap, rows), jnp.float32)
    for choice in range(route_e.shape[0]):
        match = route_e[choice:choice + 1, :].astype(jnp.float32) == owner
        named += jnp.where(match, 1.0, 0.0)
        share += jnp.where(match, route_w[choice:choice + 1, :], 0.0)
    earlier = lax.broadcasted_iota(jnp.int32, (rows, rows), 0) < lax.broadcasted_iota(
        jnp.int32, (rows, rows), 1
    )
    rank = jnp.dot(
        named.astype(jnp.bfloat16),
        jnp.where(earlier, 1.0, 0.0).astype(jnp.bfloat16),
        preferred_element_type=jnp.float32,
    )
    held = jnp.where(rank == slot, named, 0.0)
    placed[...] = held.astype(jnp.bfloat16).reshape(sp, cap, rows)
    mix[...] = share * held

    sends = []

    def begin(copy):
        copy.start()
        sends.append(copy)

    pieces = z_send.shape[1]
    span = local // pieces

    def along(block, to, d, i):
        part_of = kv.at[block, i * span:(i + 1) * span]
        return remote(part_of, part_of, z_send.at[d, i], z_recv.at[d, i], to, t)

    def across(block, d, i):
        part_of = kv.at[block, i * span:(i + 1) * span]
        return remote(part_of, part_of, x_send.at[d, i], x_recv.at[d, i], px, t)

    for copy in fetches[:3]:
        copy.wait()
    pl.semaphore_wait(barrier, len(peers))
    for d in (2, 1):
        @pl.when(z + d < lanes)
        def _():
            for i in range(pieces):
                along(s, s + 2 * d, d, i).start()

    @pl.when(x == 0)
    def _():
        for i in range(pieces):
            across(s, 0, i).start()

    def lend(n, r):
        to = flipped(t, r)
        columns = slice(n * chunk, (n + 1) * chunk)
        return remote(
            down.at[:, columns], moved.at[n, r - 1], d_send.at[n, r - 1], d_recv.at[n, r - 1],
            s, to,
        )

    def relend(n):
        return remote(
            moved.at[n, 1], moved.at[n, 2], d_send.at[n, 2], d_recv.at[n, 2], s, core
        )

    def table(j):
        there = flipped(s, 2 * j)
        pair_of = pl.ds(2 * lax.div(there, 2), 2)
        return remote(
            placed.at[pair_of], tables.at[j], t_send.at[j], t_recv.at[j], there, t
        )

    for j in range(1, lanes):
        begin(table(j))

    fetches[3].wait()
    for n in range(early):
        begin(lend(n, 2))
    for n in range(chunks):
        begin(lend(n, 1))

    for level, order in ((1, (1,)), (2, (2, 1)), (3, (1, 2, 3))):
        @pl.when(z == level)
        def _():
            for d in order:
                for i in range(pieces):
                    along(s - 2 * d, s, d, i).wait_recv()
                    if level + d == 4 and d == 2:
                        along(s - 2 * d, s + 2, 3, i).start()
                    across(s - 2 * d, d, i).start()
            for d in order:
                for i in range(pieces):
                    across(px - 2 * d, d, i).wait_recv()

    @pl.when(x == 1)
    def _():
        for i in range(pieces):
            across(px, 0, i).wait_recv()

    for copy in fetches[4:6]:
        copy.wait()
    length = sp * local
    key_pos = lax.broadcasted_iota(jnp.int32, (local, length), 1)
    query_pos = s * local + lax.broadcasted_iota(jnp.int32, (local, length), 0)
    allowed = key_pos <= query_pos
    per_key = heads // kv_heads
    for h in range(heads):
        g = h // per_key
        values = kv[:, :, 2 * kw + g * 2 * HEAD:2 * kw + (g + 1) * 2 * HEAD]
        values = values.reshape(length, 2 * HEAD)
        maps = []
        for which, q in ((0, q1), (1, q2)):
            start = which * kw + g * HEAD
            keys = kv[:, :, start:start + HEAD].reshape(length, HEAD)
            scores = lax.dot_general(
                q[:, h * HEAD:(h + 1) * HEAD],
                keys,
                (((1,), (1,)), ((), ())),
                preferred_element_type=jnp.float32,
            ) * HEAD ** (-0.5)
            scores = jnp.where(allowed, scores, -1e30)
            weights = jnp.exp(scores - jnp.max(scores, axis=-1, keepdims=True))
            totals = jnp.sum(weights, axis=-1, keepdims=True)
            added = jnp.dot(
                weights.astype(jnp.bfloat16), values, preferred_element_type=jnp.float32
            )
            maps.append(added / totals)
        difference = maps[0] - lam[h] * maps[1]
        scaled = (
            difference
            * lax.rsqrt(jnp.mean(difference * difference, axis=-1, keepdims=True) + 1e-05)
            * gain[...]
        )
        att[:, h * 2 * HEAD:(h + 1) * 2 * HEAD] = scaled.astype(jnp.bfloat16)

    fetches[6].wait()

    def share_pair(there, dy, p):
        group = flipped(core, 2) if dy else core
        return remote(
            pbuf.at[p, group], prc.at[dy, p], pc_send.at[dy, p], pc_recv.at[dy, p], s, core
        )

    def share_plane(p):
        return remote(pcs.at[p], pry.at[p], py_send.at[p], py_recv.at[p], s, plane_peer)

    parts = pbuf.shape[0]
    part_width = width // parts
    for p in range(parts + 1):
        if p < parts:
            piece = jnp.dot(
                att[...],
                ow[:, p * part_width:(p + 1) * part_width],
                preferred_element_type=jnp.float32,
            )
            pbuf[p] = piece.astype(jnp.bfloat16).reshape(tp, rows, part_width)
            for dy in (1, 0):
                begin(share_pair(None, dy, p))
        if p >= 1:
            share_pair(None, 1, p - 1).wait_recv()
            pcs[p - 1] = (
                pbuf[p - 1, plane_peer].astype(jnp.float32) + prc[1, p - 1].astype(jnp.float32)
            ).astype(jnp.bfloat16)
            begin(share_plane(p - 1))
    for n in range(early, chunks):
        begin(lend(n, 2))
    fetches[7].wait()
    summed = jnp.zeros((rows, 1), jnp.float32)
    for p in range(parts):
        columns = slice(p * part_width, (p + 1) * part_width)
        share_pair(None, 0, p).wait_recv()
        piece = pbuf[p, t].astype(jnp.float32) + prc[0, p].astype(jnp.float32)
        piece = piece + res[:, columns].astype(jnp.float32)
        share_plane(p).wait_recv()
        piece = piece + pry[p].astype(jnp.float32)
        total[:, columns] = piece
        summed += jnp.sum(piece, axis=-1, keepdims=True)
    centered = total[...] - summed / width
    variance = jnp.mean(centered * centered, axis=-1, keepdims=True)
    held_rows[0] = (centered * lax.rsqrt(variance + 1e-05) * ngain[...]).astype(jnp.bfloat16)

    tile = math.gcd(width, 1024)

    inner = (z > 0) & (z < lanes - 1)

    def to_row(j):
        return remote(
            held_rows.at[0], held_rows.at[j], r_send.at[j], r_recv.at[j], flipped(s, 2 * j), t
        )

    def pass_row():
        return remote(
            held_rows.at[2], held_rows.at[3], r_send.at[0], r_recv.at[3], flipped(s, 2), t
        )

    begin(to_row(1))
    begin(to_row(2))

    @pl.when(inner)
    def _():
        to_row(3).start()

    def arrive(j):
        k = 2 * j + 1
        return remote(outg.at[j], tok.at[k, t], a_send.at[k], a_recv.at[k], px, t)

    def select(j):
        if j:
            to_row(j).wait_recv()
        if j == 2:
            @pl.when(inner)
            def _():
                pass_row().start()
        if j:
            table(j).wait_recv()
            mine, other = tables[j, x], tables[j, 1 - x]
        else:
            mine, other = placed[s], placed[px]
        both = jnp.concatenate([mine, other], axis=0)
        for n in range(width // tile):
            columns = slice(n * tile, (n + 1) * tile)
            piece = jnp.dot(both, held_rows[j, :, columns], preferred_element_type=jnp.float32)
            piece = piece.astype(jnp.bfloat16)
            tok[2 * j, t, :, columns] = piece[:cap]
            outg[j, :, columns] = piece[cap:]
        begin(arrive(j))

    def plane(k):
        return remote(
            tok.at[k, t], tok.at[k, t], y_send.at[k], y_recv.at[k], s, plane_peer
        )

    def pair(k, dy):
        mine = plane_peer if dy else t
        return remote(
            tok.at[k, mine], tok.at[k, mine], c_send.at[k, dy], c_recv.at[k, dy], s, core
        )

    def back_pair(k, dy):
        group = corner if dy else core
        return remote(
            part.at[k, group], rc.at[k, dy], rc_send.at[k, dy], rc_recv.at[k, dy], s, core
        )

    def back_plane(k):
        return remote(cs.at[k], ry.at[k], ry_send.at[k], ry_recv.at[k], s, plane_peer)

    def pass_hidden(k, r):
        to = flipped(t, r)
        return remote(
            hid.at[k, to], hidr.at[k, r], h_send.at[k, r - 1], h_recv.at[k, r - 1], s, to
        )

    halves = (slice(0, shared), slice(shared, width))

    def back(k, half):
        columns = halves[half]
        return remote(
            fin.at[k, :, columns], ret.at[s, :, columns],
            ra_send.at[k, half], ra_recv.at[k, half], flipped(s, k), t,
        )

    def landed_tok(k, group, send, recv):
        remote(tok.at[k, group], tok.at[k, group], send, recv, s, core).wait_recv()

    def spread(k):
        if k % 2:
            landed_tok(k, t, a_send.at[k], a_recv.at[k])
        else:
            select(k // 2)
        begin(plane(k))
        begin(pair(k, 0))

    def relay(k):
        landed_tok(k, plane_peer, y_send.at[k], y_recv.at[k])
        begin(pair(k, 1))

    def collect(k):
        landed_tok(k, core, c_send.at[k, 0], c_recv.at[k, 0])
        landed_tok(k, corner, c_send.at[k, 1], c_recv.at[k, 1])

    def compute(k):
        token_rows = tok[k].reshape(tp * cap, width)
        gated = jnp.dot(token_rows, gate[...], preferred_element_type=jnp.float32)
        upward = jnp.dot(token_rows, up[...], preferred_element_type=jnp.float32)
        hidden = (gated / (1.0 + jnp.exp(-gated)) * upward).astype(jnp.bfloat16)
        hid[k] = hidden.reshape(tp, cap, hidden.shape[1])
        hidr[k, 0] = hid[k, t]
        for r in range(1, tp):
            begin(pass_hidden(k, r))
        step = math.gcd(own_part, 512)

        @pl.loop(0, own_part // step)
        def _(n):
            start = pl.multiple_of(n * step, step)
            piece = jnp.dot(
                hidden,
                down[:, pl.ds(pl.multiple_of(shared + start, step), step)],
                preferred_element_type=jnp.float32,
            )
            part[k, :, :, pl.ds(start, step)] = piece.astype(jnp.bfloat16).reshape(tp, cap, step)

        for dy in (1, 0):
            begin(back_pair(k, dy))

    def reduce_pair(k):
        back_pair(k, 1).wait_recv()
        cs[k] = (
            part[k, plane_peer].astype(jnp.float32) + rc[k, 1].astype(jnp.float32)
        ).astype(jnp.bfloat16)
        begin(back_plane(k))

    def finish_shared(k):
        for r in range(1, tp):
            pass_hidden(k, r).wait_recv()
        for n in range(chunks):
            columns = slice(n * chunk, (n + 1) * chunk)
            piece = jnp.dot(hidr[k, 0], down[:, columns], preferred_element_type=jnp.float32)
            for r in range(1, tp):
                piece += jnp.dot(hidr[k, r], moved[n, r - 1], preferred_element_type=jnp.float32)
            fin[k, :, columns] = piece.astype(jnp.bfloat16)
        if k:
            begin(back(k, 0))
        else:
            ret[s, :, :shared] = fin[k, :, :shared]

    def finish_own(k):
        back_pair(k, 0).wait_recv()
        whole = part[k, t].astype(jnp.float32) + rc[k, 0].astype(jnp.float32)
        back_plane(k).wait_recv()
        whole = whole + ry[k].astype(jnp.float32)
        fin[k, :, shared:] = whole.astype(jnp.bfloat16)
        if k:
            begin(back(k, 1))
        else:
            ret[s, :, shared:] = fin[k, :, shared:]

    def begin_lent(_):
        for n in range(chunks):
            lend(n, 2).wait_recv()
            begin(relend(n))
        for copy in fetches[8:10]:
            copy.wait()

    def wait_lent(_):
        for n in range(chunks):
            lend(n, 1).wait_recv()
            relend(n).wait_recv()

    actions = {
        "s": [spread], "r": [relay], "c": [collect, compute], "p": [reduce_pair],
        "f": [finish_own], "h": [finish_shared], "l": [begin_lent], "w": [wait_lent],
    }
    for action in " ".join(PLAN).split():
        for part_of in actions[action[0]]:
            part_of(int(action[1]))
    for k in range(1, sp):
        there = flipped(s, k)
        for half, columns in enumerate(halves):
            landed = ret.at[there, :, columns]
            remote(landed, landed, ra_send.at[k, half], ra_recv.at[k, half], s, core).wait_recv()

    unit = lax.broadcasted_iota(jnp.int32, (sp * cap, sp * cap), 0) == lax.broadcasted_iota(
        jnp.int32, (sp * cap, sp * cap), 1
    )
    unit = jnp.where(unit, 1.0, 0.0).astype(jnp.bfloat16)

    def turned(table):
        return lax.dot_general(
            table, unit, (((0,), (0,)), ((), ())), preferred_element_type=jnp.float32
        ).astype(jnp.bfloat16)

    high = mix[...].astype(jnp.bfloat16)
    mix_low = turned((mix[...] - high.astype(jnp.float32)).astype(jnp.bfloat16))
    mix_high = turned(high)

    leaving = []
    for n in range(width // tile):
        columns = slice(n * tile, (n + 1) * tile)
        returned = ret[:, :, columns].reshape(sp * cap, tile)
        combined = jnp.dot(mix_high, returned, preferred_element_type=jnp.float32)
        combined += jnp.dot(mix_low, returned, preferred_element_type=jnp.float32)
        result[:, columns] = (held_rows[0, :, columns].astype(jnp.float32) + combined).astype(
            jnp.bfloat16
        )
        leaving.append(
            pltpu.make_async_copy(result.at[:, columns], out.at[:, columns], o_sem.at[n])
        )
        leaving[-1].start()

    for copy in sends:
        copy.wait_send()

    @pl.when(inner)
    def _():
        to_row(3).wait_send()
        pass_row().wait_send()

    for i in range(pieces):
        for d in (2, 1):
            @pl.when(z + d < lanes)
            def _():
                along(s, s + 2 * d, d, i).wait_send()

        @pl.when(x == 0)
        def _():
            across(s, 0, i).wait_send()

        for level, order_of in ((1, (1,)), (2, (2, 1)), (3, (1, 2, 3))):
            @pl.when(z == level)
            def _():
                for d in order_of:
                    if level + d == 4 and d == 2:
                        along(s - 2 * d, s + 2, 3, i).wait_send()
                    across(s - 2 * d, d, i).wait_send()

    for copy in leaving:
        copy.wait()


def layer(
    query_one, key_one, query_two, key_two, value, lambda_head, head_gain, out_weight,
    residual, norm_gain, route_expert, route_weight, gate, up, down,
):
    sp, tp = lax.axis_size("sp"), lax.axis_size("tp")
    local = query_one.shape[0]
    heads = lambda_head.shape[0]
    kv_heads = key_one.shape[1] // HEAD
    rows, width = residual.shape
    hidden = gate.shape[1]
    cap = slots(rows, route_expert.shape[1], sp)
    lanes, parts = sp // 2, 4
    chunk = width // 8
    chunks, early = CHUNKS, EARLY
    own_part = width - chunks * chunk
    vmem = pl.BlockSpec(memory_space=pltpu.VMEM)
    hbm = pl.BlockSpec(memory_space=pl.ANY)
    smem = pl.BlockSpec(memory_space=pltpu.SMEM)
    dma = pltpu.SemaphoreType.DMA
    bf16 = jnp.bfloat16
    return pl.pallas_call(
        functools.partial(layer_kernel, sp, tp, heads, kv_heads, cap, early),
        out_shape=jax.ShapeDtypeStruct((rows, width), bf16),
        in_specs=[hbm] * 5 + [smem, vmem, hbm, hbm] + [vmem] * 3 + [hbm] * 3,
        out_specs=hbm,
        scratch_shapes=[
            pltpu.VMEM(query_one.shape, bf16),
            pltpu.VMEM(query_two.shape, bf16),
            pltpu.VMEM(residual.shape, bf16),
            pltpu.VMEM((sp, local, 4 * kv_heads * HEAD), bf16),
            pltpu.VMEM(out_weight.shape, bf16),
            pltpu.VMEM((local, heads * 2 * HEAD), bf16),
            pltpu.VMEM((parts, tp, rows, width // parts), bf16),
            pltpu.VMEM((2, parts, rows, width // parts), bf16),
            pltpu.VMEM((parts, rows, width // parts), bf16),
            pltpu.VMEM((parts, rows, width // parts), bf16),
            pltpu.VMEM((rows, width), jnp.float32),
            pltpu.VMEM((lanes, rows, width), bf16),
            pltpu.VMEM((sp, cap, rows), bf16),
            pltpu.VMEM((lanes, 2, cap, rows), bf16),
            pltpu.VMEM((sp * cap, rows), jnp.float32),
            pltpu.VMEM((width, hidden), bf16),
            pltpu.VMEM((width, hidden), bf16),
            pltpu.VMEM((hidden, width), bf16),
            pltpu.VMEM((chunks, tp - 1, hidden, chunk), bf16),
            pltpu.VMEM((sp, tp, cap, hidden), bf16),
            pltpu.VMEM((sp, tp, cap, hidden), bf16),
            pltpu.VMEM((lanes, cap, width), bf16),
            pltpu.VMEM((sp, tp, cap, width), bf16),
            pltpu.VMEM((sp, tp, cap, own_part), bf16),
            pltpu.VMEM((sp, 2, cap, own_part), bf16),
            pltpu.VMEM((sp, cap, own_part), bf16),
            pltpu.VMEM((sp, cap, own_part), bf16),
            pltpu.VMEM((sp, cap, width), bf16),
            pltpu.VMEM((sp, cap, width), bf16),
            dma((10,)), dma((lanes, 4)), dma((lanes, 4)), dma((lanes, 4)), dma((lanes, 4)),
            dma((2, parts)), dma((2, parts)), dma((parts,)), dma((parts,)),
            dma((lanes,)), dma((lanes,)), dma((lanes,)), dma((lanes,)),
            dma((chunks, tp - 1)), dma((chunks, tp - 1)), dma((sp, tp - 1)), dma((sp, tp - 1)),
            dma((sp,)), dma((sp,)), dma((sp,)), dma((sp,)), dma((sp, 2)), dma((sp, 2)),
            dma((sp, 2)), dma((sp, 2)), dma((sp,)), dma((sp,)), dma((sp, 2)), dma((sp, 2)),
            pltpu.VMEM((rows, width), bf16), dma((width // math.gcd(width, 1024),)),
        ],
        compiler_params=pltpu.CompilerParams(
            collective_id=0, has_side_effects=True, vmem_limit_bytes=VMEM_BYTES
        ),
        name="layer",
    )(
        query_one, key_one, query_two, key_two, value, lambda_head,
        head_gain[None, :], out_weight, residual, norm_gain[None, :],
        route_expert.T, route_weight.T, gate, up, down,
    )


def on_device_kernels(*arrays):
    return layer(*arrays[:12], *(weight[0] for weight in arrays[12:]))


def slots(rows, top_count, experts):
    return max(2 * rows * top_count // experts, 2)


def fits(*arrays):
    query_one, residual, route_expert = arrays[0], arrays[8], arrays[10]
    sp, tp = lax.axis_size("sp"), lax.axis_size("tp")
    rows, top_count = route_expert.shape
    return (
        sp == 8
        and tp == 4
        and slots(rows, top_count, sp) % 16 == 0
        and rows % 16 == 0
        and query_one.shape[0] * sp <= 2048
        and residual.shape[1] % 1024 == 0
    )


def on_device(*arrays):
    if fits(*arrays):
        return on_device_kernels(*arrays)
    return on_device_collectives(*arrays)


def on_device_collectives(
    query_one,
    key_one,
    query_two,
    key_two,
    value,
    lambda_head,
    head_gain,
    out_weight,
    residual,
    norm_gain,
    route_expert,
    route_weight,
    expert_gate,
    expert_up,
    expert_down,
):
    local_tokens = query_one.shape[0]
    heads_here = lambda_head.shape[0]
    kv_here = key_one.shape[1] // HEAD
    per_key = heads_here // kv_here
    offset = lax.axis_index("sp") * local_tokens
    first_queries = query_one.reshape(local_tokens, kv_here, per_key, HEAD)
    second_queries = query_two.reshape(local_tokens, kv_here, per_key, HEAD)
    query_pos = offset + jnp.arange(local_tokens, dtype=jnp.int32)

    def initial():
        return (
            jnp.full((kv_here, per_key, local_tokens), -1e30, jnp.float32),
            jnp.zeros((kv_here, per_key, local_tokens), jnp.float32),
            jnp.zeros((local_tokens, kv_here, per_key, 2 * HEAD), jnp.float32),
        )

    carried = (initial(), initial())
    key_first = lax.all_gather(key_one, "sp", axis=0, tiled=True)
    key_second = lax.all_gather(key_two, "sp", axis=0, tiled=True)
    value_rows = lax.all_gather(value, "sp", axis=0, tiled=True)
    length = key_first.shape[0]
    key_width = math.gcd(length, 1024)

    def advance(block_index, carried):
        block_start = block_index * key_width

        def attend(carried):
            first_block = lax.dynamic_slice_in_dim(key_first, block_start, key_width, 0)
            second_block = lax.dynamic_slice_in_dim(key_second, block_start, key_width, 0)
            value_block = lax.dynamic_slice_in_dim(value_rows, block_start, key_width, 0)
            first_block = first_block.reshape(key_width, kv_here, HEAD)
            second_block = second_block.reshape(key_width, kv_here, HEAD)
            value_block = value_block.reshape(key_width, kv_here, 2 * HEAD)
            key_pos = block_start + jnp.arange(key_width, dtype=jnp.int32)
            allowed = key_pos[None, :] <= query_pos[:, None]
            return (
                map_step(carried[0], first_queries, first_block, value_block, allowed),
                map_step(carried[1], second_queries, second_block, value_block, allowed),
            )

        def unchanged(carried):
            return carried

        return lax.cond(block_start <= offset + local_tokens - 1, attend, unchanged, carried)

    state_one, state_two = lax.fori_loop(0, length // key_width, advance, carried)
    difference = finish(state_one) - lambda_head.reshape(kv_here, per_key)[
        None, :, :, None
    ] * finish(state_two)
    scaled = (
        difference
        * lax.rsqrt(jnp.mean(difference * difference, axis=-1, keepdims=True) + 1e-05)
        * head_gain
    )
    attended = scaled.astype(jnp.bfloat16).reshape(local_tokens, heads_here * 2 * HEAD)
    own_rows = residual.shape[0]
    projected = lax.psum_scatter(
        jnp.dot(attended, out_weight, preferred_element_type=jnp.float32).astype(jnp.bfloat16),
        "tp",
        scatter_dimension=0,
        tiled=True,
    ).astype(jnp.float32)
    summed_in = residual.astype(jnp.float32) + projected
    centered = summed_in - jnp.mean(summed_in, axis=-1, keepdims=True)
    variance = jnp.mean(centered * centered, axis=-1, keepdims=True)
    normed = (centered * lax.rsqrt(variance + 1e-05) * norm_gain).astype(jnp.bfloat16)
    experts = lax.axis_size("sp")
    tp_count = lax.axis_size("tp")
    model_width = normed.shape[1]
    top_count = route_expert.shape[1]
    capacity = max(2 * own_rows * top_count // experts, 2)
    chosen = route_expert.reshape(own_rows * top_count)
    onehot = (chosen[:, None] == jnp.arange(experts, dtype=jnp.int32)[None, :]).astype(jnp.int32)
    slot_index = jnp.sum((jnp.cumsum(onehot, axis=0) - onehot) * onehot, axis=1)
    target = chosen * capacity + slot_index
    placed = target[:, None] == jnp.arange(experts * capacity, dtype=jnp.int32)[None, :]
    placed = jnp.any(placed.reshape(own_rows, top_count, experts * capacity), axis=1).astype(
        jnp.bfloat16
    )
    outgoing = jnp.einsum("rp,rd->pd", placed, normed, preferred_element_type=jnp.float32)
    outgoing = outgoing.astype(jnp.bfloat16).reshape(experts, capacity, model_width)
    arrived = lax.all_to_all(outgoing, "sp", split_axis=0, concat_axis=0, tiled=True)
    all_rows = lax.all_gather(arrived, "tp", axis=0, tiled=True)
    token_rows = all_rows.reshape(-1, model_width)
    gated = jnp.dot(token_rows, expert_gate[0], preferred_element_type=jnp.float32)
    upward = jnp.dot(token_rows, expert_up[0], preferred_element_type=jnp.float32)
    hidden = (jax.nn.silu(gated) * upward).astype(jnp.bfloat16)
    partial_value = (
        jnp.dot(hidden, expert_down[0], preferred_element_type=jnp.float32)
        .astype(jnp.bfloat16)
        .reshape(tp_count, experts * capacity, model_width)
    )
    summed = (
        lax.psum_scatter(partial_value, "tp", scatter_dimension=0, tiled=True)
        .astype(jnp.float32)
        .reshape(experts, capacity, model_width)
    )
    returned = lax.all_to_all(
        summed.astype(jnp.bfloat16), "sp", split_axis=0, concat_axis=0, tiled=True
    )
    picked = returned.reshape(experts * capacity, model_width)[target]
    picked = picked.reshape(own_rows, top_count, model_width).astype(jnp.float32)
    combined = jnp.sum(route_weight[:, :, None] * picked, axis=1)
    return (normed.astype(jnp.float32) + combined).astype(jnp.bfloat16)


def solution(mesh):
    in_specs = (
        P("sp", "tp"),
        P("sp", "tp"),
        P("sp", "tp"),
        P("sp", "tp"),
        P("sp", "tp"),
        P("tp"),
        P(),
        P("tp", None),
        P(("sp", "tp"), None),
        P(),
        P(("sp", "tp"), None),
        P(("sp", "tp"), None),
        P("sp", None, "tp"),
        P("sp", None, "tp"),
        P("sp", "tp", None),
    )
    out_specs = P(("sp", "tp"), None)
    return jax.shard_map(
        on_device, mesh=mesh, in_specs=in_specs, out_specs=out_specs, check_vma=False
    )
```

```python
import functools
import math

import jax
import jax.numpy as jnp
from jax import lax
from jax.experimental import pallas as pl
from jax.experimental.pallas import tpu as pltpu
from jax.sharding import PartitionSpec as P

HEAD = 128
VMEM_BYTES = 58 * 1024 * 1024
CHUNKS, EARLY = 4, 3
PLAN = (
    "s0 s1 l0 s2", "r1 c1 s4 s3", "r2 w0 p1 c2", "s5 h1 r4 p2",
    "c4 f1 h2 s6", "r5 p4 f2 c5", "h4 s7 r6 p5", "f4 c6 h5 r7",
    "p6 f5 r3 c7", "h6 r0 p7 f6", "c3 h7 p3 f7", "c0 h3 p0 f3",
    "h0 f0",
)


def map_step(carried, query_rows, key_block, value_block, allowed):
    largest, totals, running = carried
    scores = jnp.einsum(
        "qcgd,kcd->cgqk", query_rows, key_block, preferred_element_type=jnp.float32
    ) * HEAD ** (-0.5)
    scores = jnp.where(allowed[None, None], scores, -jnp.inf)
    updated = jnp.maximum(largest, jnp.max(scores, axis=-1))
    weights = jnp.exp(scores - updated[..., None])
    rescale = jnp.exp(largest - updated)
    totals = totals * rescale + jnp.sum(weights, axis=-1)
    added = jnp.einsum(
        "cgqk,kce->qcge",
        weights.astype(jnp.bfloat16),
        value_block,
        preferred_element_type=jnp.float32,
    )
    running = running * jnp.transpose(rescale, (2, 0, 1))[..., None] + added
    return (updated, totals, running)


def finish(carried):
    return carried[2] / jnp.transpose(carried[1], (2, 0, 1))[..., None]


def remote(src, dst, send, recv, sp_to, tp_to):
    return pltpu.make_async_remote_copy(
        src_ref=src,
        dst_ref=dst,
        send_sem=send,
        recv_sem=recv,
        device_id={"sp": sp_to, "tp": tp_to},
        device_id_type=pl.DeviceIdType.MESH,
    )


def flipped(index, mask):
    bit = 1
    while bit <= mask:
        if mask & bit:
            index = index + bit - 2 * bit * lax.rem(lax.div(index, bit), 2)
        bit *= 2
    return index


def layer_kernel(
    sp, tp, heads, kv_heads, cap, early,
    q1_hbm, k1_hbm, q2_hbm, k2_hbm, v_hbm, lam, gain, ow_hbm, res_hbm, ngain,
    route_e, route_w, gate_hbm, up_hbm, down_hbm, out,
    q1, q2, res, kv, ow, att, pbuf, prc, pcs, pry, total, held_rows, placed, tables, mix,
    gate, up, down, moved, hid, hidr, outg, tok, part, rc, cs, ry, fin, ret,
    f_sem, z_send, z_recv, x_send, x_recv, pc_send, pc_recv, py_send, py_recv,
    t_send, t_recv, r_send, r_recv, d_send, d_recv, h_send, h_recv, a_send, a_recv, y_send, y_recv, c_send, c_recv,
    rc_send, rc_recv, ry_send, ry_recv, ra_send, ra_recv, result, o_sem,
):
    s = lax.axis_index("sp")
    t = lax.axis_index("tp")
    z, x = lax.div(s, 2), lax.rem(s, 2)
    y, c = lax.div(t, 2), lax.rem(t, 2)
    lanes = sp // 2
    px = flipped(s, 1)
    core = flipped(t, 1)
    plane_peer = flipped(t, 2)
    corner = flipped(t, 3)
    local = q1.shape[0]
    rows, width = out.shape
    kw = kv_heads * HEAD
    chunks, chunk = moved.shape[0], moved.shape[3]
    shared = chunks * chunk
    own_part = width - shared

    barrier = pltpu.get_barrier_semaphore()
    peers = [(flipped(s, k), t) for k in range(1, sp)]
    peers += [(s, flipped(t, r)) for r in range(1, tp)]
    for sp_to, tp_to in peers:
        pl.semaphore_signal(
            barrier,
            inc=1,
            device_id={"sp": sp_to, "tp": tp_to},
            device_id_type=pl.DeviceIdType.MESH,
        )
    sources = [
        (k1_hbm, kv.at[s, :, 0:kw]), (k2_hbm, kv.at[s, :, kw:2 * kw]),
        (v_hbm, kv.at[s, :, 2 * kw:4 * kw]), (down_hbm, down), (q1_hbm, q1), (q2_hbm, q2),
        (ow_hbm, ow), (res_hbm, res), (gate_hbm, gate), (up_hbm, up),
    ]
    fetches = [
        pltpu.make_async_copy(src, dst, f_sem.at[i]) for i, (src, dst) in enumerate(sources)
    ]
    for copy in fetches:
        copy.start()
    for block in range(1, sp):
        @pl.when(block > s)
        def _():
            kv[block] = jnp.zeros(kv.shape[1:], kv.dtype)

    places = lax.broadcasted_iota(jnp.int32, (sp * cap, rows), 0).astype(jnp.float32)
    owner = jnp.floor((places + 0.5) / cap)
    slot = places - owner * cap
    named = jnp.zeros((sp * cap, rows), jnp.float32)
    share = jnp.zeros((sp * cap, rows), jnp.float32)
    for choice in range(route_e.shape[0]):
        match = route_e[choice:choice + 1, :].astype(jnp.float32) == owner
        named += jnp.where(match, 1.0, 0.0)
        share += jnp.where(match, route_w[choice:choice + 1, :], 0.0)
    earlier = lax.broadcasted_iota(jnp.int32, (rows, rows), 0) < lax.broadcasted_iota(
        jnp.int32, (rows, rows), 1
    )
    rank = jnp.dot(
        named.astype(jnp.bfloat16),
        jnp.where(earlier, 1.0, 0.0).astype(jnp.bfloat16),
        preferred_element_type=jnp.float32,
    )
    held = jnp.where(rank == slot, named, 0.0)
    placed[...] = held.astype(jnp.bfloat16).reshape(sp, cap, rows)
    mix[...] = share * held

    sends = []

    def begin(copy):
        copy.start()
        sends.append(copy)

    pieces = z_send.shape[1]
    span = local // pieces

    def along(block, to, d, i):
        part_of = kv.at[block, i * span:(i + 1) * span]
        return remote(part_of, part_of, z_send.at[d, i], z_recv.at[d, i], to, t)

    def across(block, d, i):
        part_of = kv.at[block, i * span:(i + 1) * span]
        return remote(part_of, part_of, x_send.at[d, i], x_recv.at[d, i], px, t)

    for copy in fetches[:3]:
        copy.wait()
    pl.semaphore_wait(barrier, len(peers))
    for d in (2, 1):
        @pl.when(z + d < lanes)
        def _():
            for i in range(pieces):
                along(s, s + 2 * d, d, i).start()

    @pl.when(x == 0)
    def _():
        for i in range(pieces):
            across(s, 0, i).start()

    def lend(n, r):
        to = flipped(t, r)
        columns = slice(n * chunk, (n + 1) * chunk)
        return remote(
            down.at[:, columns], moved.at[n, r - 1], d_send.at[n, r - 1], d_recv.at[n, r - 1],
            s, to,
        )

    def relend(n):
        return remote(
            moved.at[n, 1], moved.at[n, 2], d_send.at[n, 2], d_recv.at[n, 2], s, core
        )

    def table(j):
        there = flipped(s, 2 * j)
        pair_of = pl.ds(2 * lax.div(there, 2), 2)
        return remote(
            placed.at[pair_of], tables.at[j], t_send.at[j], t_recv.at[j], there, t
        )

    for j in range(1, lanes):
        begin(table(j))

    fetches[3].wait()
    for n in range(early):
        begin(lend(n, 2))
    for n in range(chunks):
        begin(lend(n, 1))

    for level, order in ((1, (1,)), (2, (2, 1)), (3, (1, 2, 3))):
        @pl.when(z == level)
        def _():
            for d in order:
                for i in range(pieces):
                    along(s - 2 * d, s, d, i).wait_recv()
                    if level + d == 4 and d == 2:
                        along(s - 2 * d, s + 2, 3, i).start()
                    across(s - 2 * d, d, i).start()
            for d in order:
                for i in range(pieces):
                    across(px - 2 * d, d, i).wait_recv()

    @pl.when(x == 1)
    def _():
        for i in range(pieces):
            across(px, 0, i).wait_recv()

    for copy in fetches[4:6]:
        copy.wait()
    length = sp * local
    key_pos = lax.broadcasted_iota(jnp.int32, (local, length), 1)
    query_pos = s * local + lax.broadcasted_iota(jnp.int32, (local, length), 0)
    allowed = key_pos <= query_pos
    per_key = heads // kv_heads
    for h in range(heads):
        g = h // per_key
        values = kv[:, :, 2 * kw + g * 2 * HEAD:2 * kw + (g + 1) * 2 * HEAD]
        values = values.reshape(length, 2 * HEAD)
        maps = []
        for which, q in ((0, q1), (1, q2)):
            start = which * kw + g * HEAD
            keys = kv[:, :, start:start + HEAD].reshape(length, HEAD)
            scores = lax.dot_general(
                q[:, h * HEAD:(h + 1) * HEAD],
                keys,
                (((1,), (1,)), ((), ())),
                preferred_element_type=jnp.float32,
            ) * HEAD ** (-0.5)
            scores = jnp.where(allowed, scores, -1e30)
            weights = jnp.exp(scores - jnp.max(scores, axis=-1, keepdims=True))
            totals = jnp.sum(weights, axis=-1, keepdims=True)
            added = jnp.dot(
                weights.astype(jnp.bfloat16), values, preferred_element_type=jnp.float32
            )
            maps.append(added / totals)
        difference = maps[0] - lam[h] * maps[1]
        scaled = (
            difference
            * lax.rsqrt(jnp.mean(difference * difference, axis=-1, keepdims=True) + 1e-05)
            * gain[...]
        )
        att[:, h * 2 * HEAD:(h + 1) * 2 * HEAD] = scaled.astype(jnp.bfloat16)

    fetches[6].wait()

    def share_pair(there, dy, p):
        group = flipped(core, 2) if dy else core
        return remote(
            pbuf.at[p, group], prc.at[dy, p], pc_send.at[dy, p], pc_recv.at[dy, p], s, core
        )

    def share_plane(p):
        return remote(pcs.at[p], pry.at[p], py_send.at[p], py_recv.at[p], s, plane_peer)

    parts = pbuf.shape[0]
    part_width = width // parts
    for p in range(parts + 1):
        if p < parts:
            piece = jnp.dot(
                att[...],
                ow[:, p * part_width:(p + 1) * part_width],
                preferred_element_type=jnp.float32,
            )
            pbuf[p] = piece.astype(jnp.bfloat16).reshape(tp, rows, part_width)
            for dy in (1, 0):
                begin(share_pair(None, dy, p))
        if p >= 1:
            share_pair(None, 1, p - 1).wait_recv()
            pcs[p - 1] = (
                pbuf[p - 1, plane_peer].astype(jnp.float32) + prc[1, p - 1].astype(jnp.float32)
            ).astype(jnp.bfloat16)
            begin(share_plane(p - 1))
    for n in range(early, chunks):
        begin(lend(n, 2))
    fetches[7].wait()
    summed = jnp.zeros((rows, 1), jnp.float32)
    for p in range(parts):
        columns = slice(p * part_width, (p + 1) * part_width)
        share_pair(None, 0, p).wait_recv()
        piece = pbuf[p, t].astype(jnp.float32) + prc[0, p].astype(jnp.float32)
        piece = piece + res[:, columns].astype(jnp.float32)
        share_plane(p).wait_recv()
        piece = piece + pry[p].astype(jnp.float32)
        total[:, columns] = piece
        summed += jnp.sum(piece, axis=-1, keepdims=True)
    centered = total[...] - summed / width
    variance = jnp.mean(centered * centered, axis=-1, keepdims=True)
    held_rows[0] = (centered * lax.rsqrt(variance + 1e-05) * ngain[...]).astype(jnp.bfloat16)

    tile = math.gcd(width, 1024)

    inner = (z > 0) & (z < lanes - 1)

    def to_row(j):
        return remote(
            held_rows.at[0], held_rows.at[j], r_send.at[j], r_recv.at[j], flipped(s, 2 * j), t
        )

    def pass_row():
        return remote(
            held_rows.at[2], held_rows.at[3], r_send.at[0], r_recv.at[3], flipped(s, 2), t
        )

    begin(to_row(1))
    begin(to_row(2))

    @pl.when(inner)
    def _():
        to_row(3).start()

    def arrive(j):
        k = 2 * j + 1
        return remote(outg.at[j], tok.at[k, t], a_send.at[k], a_recv.at[k], px, t)

    def select(j):
        if j:
            to_row(j).wait_recv()
        if j == 2:
            @pl.when(inner)
            def _():
                pass_row().start()
        if j:
            table(j).wait_recv()
            mine, other = tables[j, x], tables[j, 1 - x]
        else:
            mine, other = placed[s], placed[px]
        both = jnp.concatenate([mine, other], axis=0)
        for n in range(width // tile):
            columns = slice(n * tile, (n + 1) * tile)
            piece = jnp.dot(both, held_rows[j, :, columns], preferred_element_type=jnp.float32)
            piece = piece.astype(jnp.bfloat16)
            tok[2 * j, t, :, columns] = piece[:cap]
            outg[j, :, columns] = piece[cap:]
        begin(arrive(j))

    def plane(k):
        return remote(
            tok.at[k, t], tok.at[k, t], y_send.at[k], y_recv.at[k], s, plane_peer
        )

    def pair(k, dy):
        mine = plane_peer if dy else t
        return remote(
            tok.at[k, mine], tok.at[k, mine], c_send.at[k, dy], c_recv.at[k, dy], s, core
        )

    def back_pair(k, dy):
        group = corner if dy else core
        return remote(
            part.at[k, group], rc.at[k, dy], rc_send.at[k, dy], rc_recv.at[k, dy], s, core
        )

    def back_plane(k):
        return remote(cs.at[k], ry.at[k], ry_send.at[k], ry_recv.at[k], s, plane_peer)

    def pass_hidden(k, r):
        to = flipped(t, r)
        return remote(
            hid.at[k, to], hidr.at[k, r], h_send.at[k, r - 1], h_recv.at[k, r - 1], s, to
        )

    halves = (slice(0, shared), slice(shared, width))

    def back(k, half):
        columns = halves[half]
        return remote(
            fin.at[k, :, columns], ret.at[s, :, columns],
            ra_send.at[k, half], ra_recv.at[k, half], flipped(s, k), t,
        )

    def landed_tok(k, group, send, recv):
        remote(tok.at[k, group], tok.at[k, group], send, recv, s, core).wait_recv()

    def spread(k):
        if k % 2:
            landed_tok(k, t, a_send.at[k], a_recv.at[k])
        else:
            select(k // 2)
        begin(plane(k))
        begin(pair(k, 0))

    def relay(k):
        landed_tok(k, plane_peer, y_send.at[k], y_recv.at[k])
        begin(pair(k, 1))

    def collect(k):
        landed_tok(k, core, c_send.at[k, 0], c_recv.at[k, 0])
        landed_tok(k, corner, c_send.at[k, 1], c_recv.at[k, 1])

    def compute(k):
        token_rows = tok[k].reshape(tp * cap, width)
        gated = jnp.dot(token_rows, gate[...], preferred_element_type=jnp.float32)
        upward = jnp.dot(token_rows, up[...], preferred_element_type=jnp.float32)
        hidden = (gated / (1.0 + jnp.exp(-gated)) * upward).astype(jnp.bfloat16)
        hid[k] = hidden.reshape(tp, cap, hidden.shape[1])
        hidr[k, 0] = hid[k, t]
        for r in range(1, tp):
            begin(pass_hidden(k, r))
        step = math.gcd(own_part, 512)

        @pl.loop(0, own_part // step)
        def _(n):
            start = pl.multiple_of(n * step, step)
            piece = jnp.dot(
                hidden,
                down[:, pl.ds(pl.multiple_of(shared + start, step), step)],
                preferred_element_type=jnp.float32,
            )
            part[k, :, :, pl.ds(start, step)] = piece.astype(jnp.bfloat16).reshape(tp, cap, step)

        for dy in (1, 0):
            begin(back_pair(k, dy))

    def reduce_pair(k):
        back_pair(k, 1).wait_recv()
        cs[k] = (
            part[k, plane_peer].astype(jnp.float32) + rc[k, 1].astype(jnp.float32)
        ).astype(jnp.bfloat16)
        begin(back_plane(k))

    def finish_shared(k):
        for r in range(1, tp):
            pass_hidden(k, r).wait_recv()
        for n in range(chunks):
            columns = slice(n * chunk, (n + 1) * chunk)
            piece = jnp.dot(hidr[k, 0], down[:, columns], preferred_element_type=jnp.float32)
            for r in range(1, tp):
                piece += jnp.dot(hidr[k, r], moved[n, r - 1], preferred_element_type=jnp.float32)
            fin[k, :, columns] = piece.astype(jnp.bfloat16)
        if k:
            begin(back(k, 0))
        else:
            ret[s, :, :shared] = fin[k, :, :shared]

    def finish_own(k):
        back_pair(k, 0).wait_recv()
        whole = part[k, t].astype(jnp.float32) + rc[k, 0].astype(jnp.float32)
        back_plane(k).wait_recv()
        whole = whole + ry[k].astype(jnp.float32)
        fin[k, :, shared:] = whole.astype(jnp.bfloat16)
        if k:
            begin(back(k, 1))
        else:
            ret[s, :, shared:] = fin[k, :, shared:]

    def begin_lent(_):
        for n in range(chunks):
            lend(n, 2).wait_recv()
            begin(relend(n))
        for copy in fetches[8:10]:
            copy.wait()

    def wait_lent(_):
        for n in range(chunks):
            lend(n, 1).wait_recv()
            relend(n).wait_recv()

    actions = {
        "s": [spread], "r": [relay], "c": [collect, compute], "p": [reduce_pair],
        "f": [finish_own], "h": [finish_shared], "l": [begin_lent], "w": [wait_lent],
    }
    for action in " ".join(PLAN).split():
        for part_of in actions[action[0]]:
            part_of(int(action[1]))
    for k in range(1, sp):
        there = flipped(s, k)
        for half, columns in enumerate(halves):
            landed = ret.at[there, :, columns]
            remote(landed, landed, ra_send.at[k, half], ra_recv.at[k, half], s, core).wait_recv()

    unit = lax.broadcasted_iota(jnp.int32, (sp * cap, sp * cap), 0) == lax.broadcasted_iota(
        jnp.int32, (sp * cap, sp * cap), 1
    )
    unit = jnp.where(unit, 1.0, 0.0).astype(jnp.bfloat16)

    def turned(table):
        return lax.dot_general(
            table, unit, (((0,), (0,)), ((), ())), preferred_element_type=jnp.float32
        ).astype(jnp.bfloat16)

    high = mix[...].astype(jnp.bfloat16)
    mix_low = turned((mix[...] - high.astype(jnp.float32)).astype(jnp.bfloat16))
    mix_high = turned(high)

    leaving = []
    for n in range(width // tile):
        columns = slice(n * tile, (n + 1) * tile)
        returned = ret[:, :, columns].reshape(sp * cap, tile)
        combined = jnp.dot(mix_high, returned, preferred_element_type=jnp.float32)
        combined += jnp.dot(mix_low, returned, preferred_element_type=jnp.float32)
        result[:, columns] = (held_rows[0, :, columns].astype(jnp.float32) + combined).astype(
            jnp.bfloat16
        )
        leaving.append(
            pltpu.make_async_copy(result.at[:, columns], out.at[:, columns], o_sem.at[n])
        )
        leaving[-1].start()

    for copy in sends:
        copy.wait_send()

    @pl.when(inner)
    def _():
        to_row(3).wait_send()
        pass_row().wait_send()

    for i in range(pieces):
        for d in (2, 1):
            @pl.when(z + d < lanes)
            def _():
                along(s, s + 2 * d, d, i).wait_send()

        @pl.when(x == 0)
        def _():
            across(s, 0, i).wait_send()

        for level, order_of in ((1, (1,)), (2, (2, 1)), (3, (1, 2, 3))):
            @pl.when(z == level)
            def _():
                for d in order_of:
                    if level + d == 4 and d == 2:
                        along(s - 2 * d, s + 2, 3, i).wait_send()
                    across(s - 2 * d, d, i).wait_send()

    for copy in leaving:
        copy.wait()


def layer(
    query_one, key_one, query_two, key_two, value, lambda_head, head_gain, out_weight,
    residual, norm_gain, route_expert, route_weight, gate, up, down,
):
    sp, tp = lax.axis_size("sp"), lax.axis_size("tp")
    local = query_one.shape[0]
    heads = lambda_head.shape[0]
    kv_heads = key_one.shape[1] // HEAD
    rows, width = residual.shape
    hidden = gate.shape[1]
    cap = slots(rows, route_expert.shape[1], sp)
    lanes, parts = sp // 2, 4
    chunk = width // 8
    chunks, early = CHUNKS, EARLY
    own_part = width - chunks * chunk
    vmem = pl.BlockSpec(memory_space=pltpu.VMEM)
    hbm = pl.BlockSpec(memory_space=pl.ANY)
    smem = pl.BlockSpec(memory_space=pltpu.SMEM)
    dma = pltpu.SemaphoreType.DMA
    bf16 = jnp.bfloat16
    return pl.pallas_call(
        functools.partial(layer_kernel, sp, tp, heads, kv_heads, cap, early),
        out_shape=jax.ShapeDtypeStruct((rows, width), bf16),
        in_specs=[hbm] * 5 + [smem, vmem, hbm, hbm] + [vmem] * 3 + [hbm] * 3,
        out_specs=hbm,
        scratch_shapes=[
            pltpu.VMEM(query_one.shape, bf16),
            pltpu.VMEM(query_two.shape, bf16),
            pltpu.VMEM(residual.shape, bf16),
            pltpu.VMEM((sp, local, 4 * kv_heads * HEAD), bf16),
            pltpu.VMEM(out_weight.shape, bf16),
            pltpu.VMEM((local, heads * 2 * HEAD), bf16),
            pltpu.VMEM((parts, tp, rows, width // parts), bf16),
            pltpu.VMEM((2, parts, rows, width // parts), bf16),
            pltpu.VMEM((parts, rows, width // parts), bf16),
            pltpu.VMEM((parts, rows, width // parts), bf16),
            pltpu.VMEM((rows, width), jnp.float32),
            pltpu.VMEM((lanes, rows, width), bf16),
            pltpu.VMEM((sp, cap, rows), bf16),
            pltpu.VMEM((lanes, 2, cap, rows), bf16),
            pltpu.VMEM((sp * cap, rows), jnp.float32),
            pltpu.VMEM((width, hidden), bf16),
            pltpu.VMEM((width, hidden), bf16),
            pltpu.VMEM((hidden, width), bf16),
            pltpu.VMEM((chunks, tp - 1, hidden, chunk), bf16),
            pltpu.VMEM((sp, tp, cap, hidden), bf16),
            pltpu.VMEM((sp, tp, cap, hidden), bf16),
            pltpu.VMEM((lanes, cap, width), bf16),
            pltpu.VMEM((sp, tp, cap, width), bf16),
            pltpu.VMEM((sp, tp, cap, own_part), bf16),
            pltpu.VMEM((sp, 2, cap, own_part), bf16),
            pltpu.VMEM((sp, cap, own_part), bf16),
            pltpu.VMEM((sp, cap, own_part), bf16),
            pltpu.VMEM((sp, cap, width), bf16),
            pltpu.VMEM((sp, cap, width), bf16),
            dma((10,)), dma((lanes, 4)), dma((lanes, 4)), dma((lanes, 4)), dma((lanes, 4)),
            dma((2, parts)), dma((2, parts)), dma((parts,)), dma((parts,)),
            dma((lanes,)), dma((lanes,)), dma((lanes,)), dma((lanes,)),
            dma((chunks, tp - 1)), dma((chunks, tp - 1)), dma((sp, tp - 1)), dma((sp, tp - 1)),
            dma((sp,)), dma((sp,)), dma((sp,)), dma((sp,)), dma((sp, 2)), dma((sp, 2)),
            dma((sp, 2)), dma((sp, 2)), dma((sp,)), dma((sp,)), dma((sp, 2)), dma((sp, 2)),
            pltpu.VMEM((rows, width), bf16), dma((width // math.gcd(width, 1024),)),
        ],
        compiler_params=pltpu.CompilerParams(
            collective_id=0, has_side_effects=True, vmem_limit_bytes=VMEM_BYTES
        ),
        name="layer",
    )(
        query_one, key_one, query_two, key_two, value, lambda_head,
        head_gain[None, :], out_weight, residual, norm_gain[None, :],
        route_expert.T, route_weight.T, gate, up, down,
    )


def on_device_kernels(*arrays):
    return layer(*arrays[:12], *(weight[0] for weight in arrays[12:]))


def slots(rows, top_count, experts):
    return max(2 * rows * top_count // experts, 2)


def fits(*arrays):
    query_one, residual, route_expert = arrays[0], arrays[8], arrays[10]
    sp, tp = lax.axis_size("sp"), lax.axis_size("tp")
    rows, top_count = route_expert.shape
    return (
        sp == 8
        and tp == 4
        and slots(rows, top_count, sp) % 16 == 0
        and rows % 16 == 0
        and query_one.shape[0] * sp <= 2048
        and residual.shape[1] % 1024 == 0
    )


def on_device(*arrays):
    if fits(*arrays):
        return on_device_kernels(*arrays)
    return on_device_collectives(*arrays)


def on_device_collectives(
    query_one,
    key_one,
    query_two,
    key_two,
    value,
    lambda_head,
    head_gain,
    out_weight,
    residual,
    norm_gain,
    route_expert,
    route_weight,
    expert_gate,
    expert_up,
    expert_down,
):
    local_tokens = query_one.shape[0]
    heads_here = lambda_head.shape[0]
    kv_here = key_one.shape[1] // HEAD
    per_key = heads_here // kv_here
    offset = lax.axis_index("sp") * local_tokens
    first_queries = query_one.reshape(local_tokens, kv_here, per_key, HEAD)
    second_queries = query_two.reshape(local_tokens, kv_here, per_key, HEAD)
    query_pos = offset + jnp.arange(local_tokens, dtype=jnp.int32)

    def initial():
        return (
            jnp.full((kv_here, per_key, local_tokens), -1e30, jnp.float32),
            jnp.zeros((kv_here, per_key, local_tokens), jnp.float32),
            jnp.zeros((local_tokens, kv_here, per_key, 2 * HEAD), jnp.float32),
        )

    carried = (initial(), initial())
    key_first = lax.all_gather(key_one, "sp", axis=0, tiled=True)
    key_second = lax.all_gather(key_two, "sp", axis=0, tiled=True)
    value_rows = lax.all_gather(value, "sp", axis=0, tiled=True)
    length = key_first.shape[0]
    key_width = math.gcd(length, 1024)

    def advance(block_index, carried):
        block_start = block_index * key_width

        def attend(carried):
            first_block = lax.dynamic_slice_in_dim(key_first, block_start, key_width, 0)
            second_block = lax.dynamic_slice_in_dim(key_second, block_start, key_width, 0)
            value_block = lax.dynamic_slice_in_dim(value_rows, block_start, key_width, 0)
            first_block = first_block.reshape(key_width, kv_here, HEAD)
            second_block = second_block.reshape(key_width, kv_here, HEAD)
            value_block = value_block.reshape(key_width, kv_here, 2 * HEAD)
            key_pos = block_start + jnp.arange(key_width, dtype=jnp.int32)
            allowed = key_pos[None, :] <= query_pos[:, None]
            return (
                map_step(carried[0], first_queries, first_block, value_block, allowed),
                map_step(carried[1], second_queries, second_block, value_block, allowed),
            )

        def unchanged(carried):
            return carried

        return lax.cond(block_start <= offset + local_tokens - 1, attend, unchanged, carried)

    state_one, state_two = lax.fori_loop(0, length // key_width, advance, carried)
    difference = finish(state_one) - lambda_head.reshape(kv_here, per_key)[
        None, :, :, None
    ] * finish(state_two)
    scaled = (
        difference
        * lax.rsqrt(jnp.mean(difference * difference, axis=-1, keepdims=True) + 1e-05)
        * head_gain
    )
    attended = scaled.astype(jnp.bfloat16).reshape(local_tokens, heads_here * 2 * HEAD)
    own_rows = residual.shape[0]
    projected = lax.psum_scatter(
        jnp.dot(attended, out_weight, preferred_element_type=jnp.float32).astype(jnp.bfloat16),
        "tp",
        scatter_dimension=0,
        tiled=True,
    ).astype(jnp.float32)
    summed_in = residual.astype(jnp.float32) + projected
    centered = summed_in - jnp.mean(summed_in, axis=-1, keepdims=True)
    variance = jnp.mean(centered * centered, axis=-1, keepdims=True)
    normed = (centered * lax.rsqrt(variance + 1e-05) * norm_gain).astype(jnp.bfloat16)
    experts = lax.axis_size("sp")
    tp_count = lax.axis_size("tp")
    model_width = normed.shape[1]
    top_count = route_expert.shape[1]
    capacity = max(2 * own_rows * top_count // experts, 2)
    chosen = route_expert.reshape(own_rows * top_count)
    onehot = (chosen[:, None] == jnp.arange(experts, dtype=jnp.int32)[None, :]).astype(jnp.int32)
    slot_index = jnp.sum((jnp.cumsum(onehot, axis=0) - onehot) * onehot, axis=1)
    target = chosen * capacity + slot_index
    placed = target[:, None] == jnp.arange(experts * capacity, dtype=jnp.int32)[None, :]
    placed = jnp.any(placed.reshape(own_rows, top_count, experts * capacity), axis=1).astype(
        jnp.bfloat16
    )
    outgoing = jnp.einsum("rp,rd->pd", placed, normed, preferred_element_type=jnp.float32)
    outgoing = outgoing.astype(jnp.bfloat16).reshape(experts, capacity, model_width)
    arrived = lax.all_to_all(outgoing, "sp", split_axis=0, concat_axis=0, tiled=True)
    all_rows = lax.all_gather(arrived, "tp", axis=0, tiled=True)
    token_rows = all_rows.reshape(-1, model_width)
    gated = jnp.dot(token_rows, expert_gate[0], preferred_element_type=jnp.float32)
    upward = jnp.dot(token_rows, expert_up[0], preferred_element_type=jnp.float32)
    hidden = (jax.nn.silu(gated) * upward).astype(jnp.bfloat16)
    partial_value = (
        jnp.dot(hidden, expert_down[0], preferred_element_type=jnp.float32)
        .astype(jnp.bfloat16)
        .reshape(tp_count, experts * capacity, model_width)
    )
    summed = (
        lax.psum_scatter(partial_value, "tp", scatter_dimension=0, tiled=True)
        .astype(jnp.float32)
        .reshape(experts, capacity, model_width)
    )
    returned = lax.all_to_all(
        summed.astype(jnp.bfloat16), "sp", split_axis=0, concat_axis=0, tiled=True
    )
    picked = returned.reshape(experts * capacity, model_width)[target]
    picked = picked.reshape(own_rows, top_count, model_width).astype(jnp.float32)
    combined = jnp.sum(route_weight[:, :, None] * picked, axis=1)
    return (normed.astype(jnp.float32) + combined).astype(jnp.bfloat16)


def solution(mesh):
    in_specs = (
        P("sp", "tp"),
        P("sp", "tp"),
        P("sp", "tp"),
        P("sp", "tp"),
        P("sp", "tp"),
        P("tp"),
        P(),
        P("tp", None),
        P(("sp", "tp"), None),
        P(),
        P(("sp", "tp"), None),
        P(("sp", "tp"), None),
        P("sp", None, "tp"),
        P("sp", None, "tp"),
        P("sp", "tp", None),
    )
    out_specs = P(("sp", "tp"), None)
    return jax.shard_map(
        on_device, mesh=mesh, in_specs=in_specs, out_specs=out_specs, check_vma=False
    )
```
